128 devices in a mesh: sp: 32 (over z, y, core), tp: 4 (over x).
Axes of the slice: x: 4, y: 4, z: 4, core: 2. Of those that a mesh axis runs over, the one named last changes fastest.
Arguments:
- queries: bfloat16 [16384, 1024], P('sp', 'tp'), may hold values from -6 to 6
- key_heads: bfloat16 [16384, 512], P('sp', 'tp'), may hold values from -6 to 6
- value_heads: bfloat16 [16384, 512], P('sp', 'tp'), may hold values from -70 to 70
- documents: int32 [16384], P('sp'), may hold values from 0 to 8, never falling along the last dimension, each value on 1 to 10240 neighbouring positions
- query_gain: float32 [128], replicated, may hold values from 0.1 to 8
- key_gain: float32 [128], replicated, may hold values from 0.1 to 8
- out_gain: float32 [1024], replicated, may hold values from 0.1 to 1.9
- out_proj: bfloat16 [1024, 2048], replicated, may hold values from -0.1875 to 0.1875
- residual: bfloat16 [16384, 2048], P(('sp', 'tp')), may hold values from -6 to 6
- mid_gain: float32 [2048], replicated, may hold values from 0.1 to 1.9
- mid_bias: float32 [2048], replicated, may hold values from -1.5 to 1.5
- routes: int32 [16384, 2], P(('sp', 'tp')), may hold values from 0 to 127, all different within a row; in each aligned block of 128 rows (0 to 127, 128 to 255, ...) at most 4 rows name the same one
- route_weights: float32 [16384, 2], P(('sp', 'tp')), may hold values from 0.2 to 2
- expert_gate: bfloat16 [128, 2048, 512], P(('sp', 'tp')), may hold values from -0.125 to 0.125
- expert_up: bfloat16 [128, 2048, 512], P(('sp', 'tp')), may hold values from -0.125 to 0.125
- expert_down: bfloat16 [128, 512, 2048], P(('sp', 'tp')), may hold values from -0.25 to 0.25
- final_gain: float32 [2048], replicated, may hold values from 0.1 to 1.9
- final_bias: float32 [2048], replicated, may hold values from -1.5 to 1.5
Outputs:
- layer_out: bfloat16 [16384, 2048], P(('sp', 'tp'))
The draws below stay inside these ranges and needn't reach their ends.
Inputs may be any that keep to these rules, and one draw needn't show every extreme that they name: `documents`: never falls along the sequence; each document holds 1 to 10240 positions and one holds exactly 10240. `routes`: each row names 2 different experts; among the rows of one device (aligned blocks of 128 rows) no expert is named more than 4 times, and exactly 4 times in some block.
All inputs are finite; a program needn't handle non-finite values.
Results may differ from the reference program's by a relative error of at most 0.014.
The reference program's roundings to bfloat16 on the way count: a program that leaves them out, or rounds other values in their place, can miss the bound.
Values may be sent and summed in bfloat16 or wider, within the bound.
A program may use at most 128 MiB of HBM per device.

```python
import math
import jax
import jax.numpy as jnp
import numpy as np
from jax import lax

D = 2048
HEAD = 128
QH = 8
KVH = 4
GRID = 64
DE = 512
TOP_K = 2
TOKENS = 16384
ROWS = 128
EXPERTS = 128
CAP = 4
DOCS = 9
DOC_MOST = 10240
N_SP = 32
N_TP = 4


def drawn_keys(key):
    sub_key = jax.random.fold_in(key, 202)
    drawn = jnp.clip(jax.random.normal(sub_key, (TOKENS, KVH * HEAD), jnp.float32), -6.0, 6.0)
    return drawn


def draw_key_heads(key, part):
    return drawn_keys(key).astype(jnp.bfloat16)


def draw_queries(key, part):
    sub_key = jax.random.fold_in(key, 301)
    drawn = jnp.clip(jax.random.normal(sub_key, (TOKENS, QH * HEAD), jnp.float32), -6.0, 6.0)
    return drawn.astype(jnp.bfloat16)


def draw_value_heads(key, part):
    sub_key = jax.random.fold_in(key, 501)
    head_index = jnp.arange(KVH, dtype=jnp.float32)
    head_scale = jnp.repeat(4.0 ** (head_index / (KVH - 1)), HEAD)
    drawn = jnp.clip(jax.random.normal(sub_key, (TOKENS, KVH * HEAD), jnp.float32), -4.0, 4.0)
    return (drawn * head_scale[None, :]).astype(jnp.bfloat16)


def gain_values(key):
    return jnp.clip(1.0 + 0.18 * jax.random.normal(key, (HEAD,), jnp.float32), 0.1, 1.9)


def draw_query_gain(key, part):
    return gain_values(jax.random.fold_in(key, 401))


def draw_key_gain(key, part):
    return gain_values(jax.random.fold_in(key, 402))


def levels(stream_key, shape, shards, smallest, largest):
    loudness, own = 1.0, jax.random.fold_in(stream_key, 6)
    for position, shards_of in shards:
        heights = jnp.exp(jax.random.uniform(jax.random.fold_in(own, position), (shards_of,), jnp.float32, smallest / len(shards), largest / len(shards)))
        loudness = loudness * jnp.repeat(heights, shape[position] // shards_of).reshape([-1 if axis == position else 1 for axis in range(len(shape))])
    return loudness


def profile(amount, total, limit, skew):
    portions = [(1 << 20) // math.isqrt(rank ** skew) + 1 for rank in range(2, amount + 1)]
    surplus, holding = total - limit - (amount - 1), [1] * (amount - 1)
    while surplus > 0:
        movable = [i for i in range(amount - 1) if holding[i] < limit]
        whole, left = sum([portions[i] for i in movable]), surplus
        for i in movable:
            extra = min(limit - holding[i], max(1, left * portions[i] // whole), surplus)
            holding[i] = holding[i] + extra
            surplus = surplus - extra
    return np.array([limit] + holding)


def uneven_parts(rng, amount, total, limit, skew):
    if amount == 2:
        one = jax.random.randint(rng, (), max(1, total - limit), min(limit, total - 1) + 1)
        return jnp.stack([one, total - one])
    tallies = jnp.asarray(profile(amount, total, limit, skew), jnp.int32)
    twos = (amount - 1) // 2
    donor, taker = tallies[1:1 + 2 * twos:2], tallies[2:2 + 2 * twos:2]
    room = jnp.minimum(donor - 1, limit - taker)
    passed = jax.random.randint(jax.random.fold_in(rng, 1), (twos,), 0, 1 << 20) % (room + 1)
    tallies = tallies.at[1:1 + 2 * twos:2].set(donor - passed).at[2:2 + 2 * twos:2].set(taker + passed)
    return tallies[jax.random.permutation(jax.random.fold_in(rng, 2), amount)]


def assign_block(key, own, number, rows, number_of, top, limit, slope):
    order = jax.random.permutation(key, number_of)
    crowded, common = portions_of(number_of, rows * top, limit, slope, True), portions_of(number_of, rows * top, limit, slope, False)
    places = jnp.arange(number_of)

    def named(sizes, offset_by):
        used = int((sizes > 0).sum())
        fixed = max(1, used // 4)
        passed = fixed + (places - fixed + offset_by * (used - fixed)) % max(1, number_of - fixed)
        return jnp.zeros((number_of,), jnp.int32).at[order[jnp.where(places < fixed, places, passed)]].set(jnp.asarray(sizes, jnp.int32))

    sizes = jnp.where(number % 4 == 0, named(crowded, number // 4), named(common, number - number // 4 - 1))
    mixed = jax.random.permutation(jax.random.fold_in(own, 3), number_of)
    giver, receiver = mixed[0:number_of // 2 * 2:2], mixed[1:number_of // 2 * 2:2]
    slack = jnp.minimum(sizes[giver] - 1, limit - sizes[receiver]) // 2
    slack = jnp.where((giver == order[0]) | (receiver == order[0]) | (sizes[receiver] == 0), 0, jnp.maximum(slack, 0))
    passed = jax.random.randint(jax.random.fold_in(own, 4), (number_of // 2,), 0, 1 << 20) % (slack + 1)
    sizes = sizes.at[giver].add(-passed).at[receiver].add(passed)
    items = jnp.searchsorted(jnp.cumsum(sizes), jnp.arange(rows * top), side="right").astype(jnp.int32)
    table = items.reshape(top, rows).T
    table = table[jax.random.permutation(jax.random.fold_in(own, 1), rows)]
    offset_by = jax.random.randint(jax.random.fold_in(own, 2), (rows, 1), 0, top)
    return jnp.take_along_axis(table, (jnp.arange(top)[None, :] + offset_by) % top, axis=1)


def portions_of(amount, total, most, lean, full):
    loads = [(1 << 20) // math.isqrt(standing ** lean) + 1 for standing in range(1, amount + 1)]
    largest = most if full else min(most, max(-(-total // amount), total * loads[0] // sum(loads)))
    least = 1 if total - largest >= amount - 1 else 0
    given, spare = [largest] + [least] * (amount - 1), total - largest - least * (amount - 1)
    while spare > 0:
        candidates = [i for i in range(1, amount) if given[i] < largest] or [i for i in range(1, amount) if given[i] < most]
        mass, left = sum([loads[i] for i in candidates]), spare
        for i in candidates:
            extra = min(most - given[i], max(1, left * loads[i] // mass), spare)
            given[i] = given[i] + extra
            spare = spare - extra
    return np.array(given)


def gaussian(stream_key, extent, deviation, limit, shards=(), kind=jnp.bfloat16):
    array = deviation * jax.random.normal(stream_key, extent, jnp.float32)
    if shards:
        array = array * levels(stream_key, extent, shards, -0.22, 0.18)
    return jnp.clip(array, -limit, limit).astype(kind)


def setup_inputs(seed: int = 0) -> dict:
    streams_of = jax.random.split(jax.random.key(seed), 19)
    queries = draw_queries(jax.random.fold_in(streams_of[18], 71), 0)
    key_heads = draw_key_heads(jax.random.fold_in(streams_of[18], 71), 0)
    value_heads = draw_value_heads(jax.random.fold_in(streams_of[18], 71), 0)
    documents = jnp.searchsorted(jnp.cumsum(uneven_parts(streams_of[3], DOCS, TOKENS, DOC_MOST, 1)), jnp.arange(TOKENS), side="right").astype(jnp.int32)
    query_gain = draw_query_gain(jax.random.fold_in(streams_of[18], 71), 0)
    key_gain = draw_key_gain(jax.random.fold_in(streams_of[18], 71), 0)
    out_gain = jnp.clip(1.0 + 0.18 * jax.random.normal(streams_of[6], (QH * HEAD,), jnp.float32), 0.1, 1.9)
    out_proj = gaussian(streams_of[7], (QH * HEAD, D), (QH * HEAD) ** -0.5, 0.1875)
    residual = gaussian(streams_of[8], (TOKENS, D), 1.0, 6.0, ((0, 128),))
    mid_gain = jnp.clip(1.0 + 0.18 * jax.random.normal(streams_of[9], (D,), jnp.float32), 0.1, 1.9)
    mid_bias = gaussian(streams_of[10], (D,), 0.3, 1.5, (), jnp.float32)
    routes_keys = jax.random.split(jax.random.fold_in(streams_of[11], 1), TOKENS // ROWS)
    routes_turns = jax.random.permutation(jax.random.fold_in(streams_of[11], 3), TOKENS // ROWS)
    routes = jax.vmap(lambda own, number: assign_block(jax.random.fold_in(streams_of[11], 2), own, number, ROWS, EXPERTS, TOP_K, CAP, 2))(routes_keys, routes_turns).reshape((TOKENS, TOP_K))
    route_weights = jnp.clip(jnp.exp(math.log(2.0) - 2.3025851 * jax.random.uniform(streams_of[12], (TOKENS, TOP_K), jnp.float32) ** levels(streams_of[12], (TOKENS, TOP_K), ((0, 128),), -0.2, 0.2)), 0.2, 2.0)
    expert_gate = gaussian(streams_of[13], (EXPERTS, D, DE), D ** -0.5, 0.125, ((0, 128),))
    expert_up = gaussian(streams_of[14], (EXPERTS, D, DE), D ** -0.5, 0.125, ((0, 128),))
    expert_down = gaussian(streams_of[15], (EXPERTS, DE, D), DE ** -0.5, 0.25, ((0, 128),))
    final_gain = jnp.clip(1.0 + 0.18 * jax.random.normal(streams_of[16], (D,), jnp.float32), 0.1, 1.9)
    final_bias = gaussian(streams_of[17], (D,), 0.3, 1.5, (), jnp.float32)
    return dict(queries=queries, key_heads=key_heads, value_heads=value_heads, documents=documents, query_gain=query_gain, key_gain=key_gain, out_gain=out_gain, out_proj=out_proj, residual=residual, mid_gain=mid_gain, mid_bias=mid_bias, routes=routes, route_weights=route_weights, expert_gate=expert_gate, expert_up=expert_up, expert_down=expert_down, final_gain=final_gain, final_bias=final_bias)


eps_norm = 1e-06
alpha_mix = 8.0 ** 0.25
theta_base = 10000.0

def rotary_tables(row_total, offset):
    positions = offset + jnp.arange(row_total, dtype=jnp.int32)
    grid_row = (positions // GRID).astype(jnp.float32)
    grid_col = (positions % GRID).astype(jnp.float32)
    pair_count = HEAD // 4
    inv_freq = theta_base ** (-jnp.arange(pair_count, dtype=jnp.float32) / pair_count)
    angles = jnp.concatenate([grid_row[:, None] * inv_freq[None, :], grid_col[:, None] * inv_freq[None, :]], axis=1)
    return (jnp.cos(angles), jnp.sin(angles))

def normed_rotated(heads_in, gain_vec, cosine_table, sine_table):
    values = heads_in.astype(jnp.float32)
    inv_rms = lax.rsqrt(lax.optimization_barrier(jnp.mean(values * values, axis=-1, keepdims=True)) + eps_norm)
    values = values * inv_rms * gain_vec
    half_dim = HEAD // 2
    first_half = values[..., :half_dim]
    second_half = values[..., half_dim:]
    cosine_part = cosine_table[:, None, :]
    sine_part = sine_table[:, None, :]
    turned = jnp.concatenate([first_half * cosine_part - second_half * sine_part, second_half * cosine_part + first_half * sine_part], axis=-1)
    return turned.astype(jnp.bfloat16)

def layer_norm(stream, gain_vec, bias_vec):
    center = lax.optimization_barrier(jnp.mean(stream, axis=-1, keepdims=True))
    spread = lax.optimization_barrier(jnp.mean(jnp.square(stream - center), axis=-1, keepdims=True))
    return (stream - center) * lax.rsqrt(spread + eps_norm) * gain_vec + bias_vec

def reference(queries, key_heads, value_heads, documents, query_gain, key_gain, out_gain, out_proj, residual, mid_gain, mid_bias, routes, route_weights, expert_gate, expert_up, expert_down, final_gain, final_bias):
    cosine_table, sine_table = rotary_tables(TOKENS, 0)
    grouped = QH // KVH
    query_rot = normed_rotated(queries.reshape(TOKENS, QH, HEAD), query_gain, cosine_table, sine_table).reshape(TOKENS, KVH, grouped, HEAD)
    key_rot = normed_rotated(key_heads.reshape(TOKENS, KVH, HEAD), key_gain, cosine_table, sine_table).astype(jnp.float32)
    value_all = value_heads.reshape(TOKENS, KVH, HEAD).astype(jnp.float32)
    block_rows = math.gcd(TOKENS, 512)

    def query_block(number):
        first_row = number * block_rows
        query_part = lax.dynamic_slice_in_dim(query_rot, first_row, block_rows, 0).astype(jnp.float32)
        doc_part = lax.dynamic_slice_in_dim(documents, first_row, block_rows, 0)
        scores = jnp.einsum('qkgd,tkd->kgqt', query_part, key_rot) * HEAD ** (-0.5)
        allowed = (doc_part[:, None] == documents[None, :])[None, None]
        scores = jnp.where(allowed, scores, -1e+30)
        row_max = lax.optimization_barrier(jnp.max(scores, axis=-1, keepdims=True))
        weights = jnp.where(allowed, jnp.exp(scores - row_max), 0.0)
        totals = lax.optimization_barrier(jnp.sum(weights, axis=-1))
        rounded = lax.optimization_barrier(weights.astype(jnp.bfloat16)).astype(jnp.float32)
        summed = jnp.einsum('kgqt,tkd->kgqd', rounded, value_all) / totals[..., None]
        return jnp.transpose(summed, (2, 0, 1, 3)).reshape(block_rows, QH * HEAD).astype(jnp.bfloat16)
    attention = lax.map(query_block, jnp.arange(TOKENS // block_rows, dtype=jnp.int32))
    attention = attention.reshape(TOKENS, QH * HEAD)
    attn_float = attention.astype(jnp.float32)
    mean_square = lax.optimization_barrier(jnp.mean(attn_float * attn_float, axis=1, keepdims=True))
    scaled = (attn_float * out_gain).astype(jnp.bfloat16)
    projected = jnp.dot(scaled, out_proj, preferred_element_type=jnp.float32) * lax.rsqrt(mean_square + eps_norm)
    middle = layer_norm(alpha_mix * residual.astype(jnp.float32) + projected, mid_gain, mid_bias).astype(jnp.bfloat16)
    flat_routes = routes.reshape(-1).astype(jnp.int32)
    pair_total = flat_routes.shape[0]
    receive = N_SP * N_TP * CAP
    sorted_order = jnp.argsort(flat_routes, stable=True).astype(jnp.int32)
    counts = lax.optimization_barrier(jnp.sum((flat_routes[:, None] == jnp.arange(EXPERTS, dtype=jnp.int32)[None, :]).astype(jnp.int32), axis=0))
    starts = jnp.cumsum(counts) - counts
    inverse = jnp.zeros((pair_total,), jnp.int32).at[sorted_order].set(jnp.arange(pair_total, dtype=jnp.int32))
    token_of = sorted_order // TOP_K

    def expert_pass(expert):
        slot_index = starts[expert] + jnp.arange(receive, dtype=jnp.int32)
        live_rows = slot_index < starts[expert] + counts[expert]
        source_rows = middle[token_of[jnp.minimum(slot_index, pair_total - 1)]]
        picked = jnp.where(live_rows[:, None], source_rows, jnp.zeros((), jnp.bfloat16))
        gate_part = jnp.dot(picked, expert_gate[expert], preferred_element_type=jnp.float32)
        up_part = jnp.dot(picked, expert_up[expert], preferred_element_type=jnp.float32)
        hidden = (jax.nn.silu(gate_part) * up_part).astype(jnp.bfloat16)
        return jnp.dot(hidden, expert_down[expert], preferred_element_type=jnp.float32).astype(jnp.bfloat16)
    served = lax.map(expert_pass, jnp.arange(EXPERTS, dtype=jnp.int32)).reshape(EXPERTS * receive, D)
    slot_rows = flat_routes * receive + (inverse - starts[flat_routes])
    gathered = served[slot_rows].astype(jnp.float32).reshape(TOKENS, TOP_K, D)
    routed = lax.optimization_barrier(jnp.sum(gathered * route_weights[:, :, None], axis=1))
    return layer_norm(alpha_mix * middle.astype(jnp.float32) + routed, final_gain, final_bias).astype(jnp.bfloat16)
```

```python
import functools
import math

import jax
import jax.numpy as jnp
import numpy as np
from jax import lax
from jax.experimental import pallas as pl
from jax.experimental.pallas import tpu as pltpu
from jax.sharding import PartitionSpec as P

HEAD = 128
GRID = 64
KEY_BLOCK = 1152
ALIGN = 128

eps_norm = 1e-06
alpha_mix = 8.0**0.25
theta_base = 10000.0
LOG2_SCALE = HEAD ** (-0.5) * math.log2(math.e)

ANY = pl.BlockSpec(memory_space=pl.ANY)
VMEM = pl.BlockSpec(memory_space=pltpu.VMEM)


def rotary_tables(row_total, offset):
    positions = offset + jnp.arange(row_total, dtype=jnp.int32)
    grid_row = (positions // GRID).astype(jnp.float32)
    grid_col = (positions % GRID).astype(jnp.float32)
    pair_count = HEAD // 4
    inv_freq = theta_base ** (-jnp.arange(pair_count, dtype=jnp.float32) / pair_count)
    angles = jnp.concatenate(
        [grid_row[:, None] * inv_freq[None, :], grid_col[:, None] * inv_freq[None, :]], axis=1
    )
    cosine, sine = jnp.cos(angles), jnp.sin(angles)
    return jnp.concatenate([cosine, cosine], axis=1), jnp.concatenate([-sine, sine], axis=1)


def turn(values, gain, cosine, sine):
    inv_rms = lax.rsqrt(jnp.mean(values * values, axis=-1, keepdims=True) + eps_norm)
    values = values * inv_rms * gain
    swapped = pltpu.roll(values, HEAD // 2, 1)
    return (values * cosine + swapped * sine).astype(jnp.bfloat16)


def key_kernel(key_ref, value_ref, docs_ref, gain_ref, cos_ref, sin_ref, out_ref):
    rows = key_ref.shape[0]
    out_ref[0:rows, 0:HEAD] = turn(
        key_ref[...].astype(jnp.float32), gain_ref[...], cos_ref[...], sin_ref[...]
    )
    out_ref[0:rows, HEAD:] = value_ref[...]
    out_ref[rows:, :] = jnp.zeros((out_ref.shape[0] - rows, out_ref.shape[1]), jnp.bfloat16)
    docs = docs_ref[...].astype(jnp.float32)
    padded = jnp.concatenate([docs, jnp.zeros((16 - docs.shape[0], docs.shape[1]), jnp.float32)], axis=0)
    out_ref[rows:, :] = padded.astype(jnp.bfloat16)


def query_kernel(query_ref, gain_ref, cos_ref, sin_ref, out_ref):
    for head in range(out_ref.shape[0]):
        out_ref[head] = turn(
            query_ref[:, head * HEAD : (head + 1) * HEAD].astype(jnp.float32),
            gain_ref[...],
            cos_ref[...],
            sin_ref[...],
        )


def attention_kernel(shards, rows, tile, q_ref, docs_ref, kv_ref, out_ref, k_buf, v_buf, d_buf, start_buf, end_buf, acc, top, sem):
    heads = q_ref.shape[0]
    total_keys = shards * rows
    doc_copy = pltpu.make_async_copy(kv_ref.at[:, pl.ds(rows, 16), :], d_buf, sem.at[2 * shards])
    doc_copy.start()
    v_buf[:, HEAD:] = jnp.ones((v_buf.shape[0], HEAD), jnp.bfloat16)
    v_buf[total_keys:, 0:HEAD] = jnp.zeros((KEY_BLOCK, HEAD), jnp.bfloat16)
    doc_copy.wait()
    all_docs = d_buf[:, 0:8, :].astype(jnp.float32).astype(jnp.int32)[:, 0:2, :]
    docs_here = docs_ref[...]
    half = rows // 2

    counts = [
        jnp.sum(jnp.sum((all_docs < d).astype(jnp.float32), axis=(0, 1), keepdims=False)[None, :], axis=1, keepdims=True)
        for d in range(1, 9)
    ]
    counts = [jnp.zeros((1, 1), jnp.float32)] + counts + [jnp.full((1, 1), float(total_keys), jnp.float32)]
    bounds = []
    for t in range(rows // tile):
        per_row = half // tile
        mine = docs_here[t // per_row : t // per_row + 1, (t % per_row) * tile : (t % per_row + 1) * tile]
        start_row = jnp.zeros(mine.shape, jnp.float32)
        end_row = jnp.zeros(mine.shape, jnp.float32)
        for d in range(9):
            start_row = jnp.where(mine == d, counts[d], start_row)
            end_row = jnp.where(mine == d, counts[d + 1], end_row)
        for row, buf in ((start_row, start_buf), (end_row, end_buf)):
            column = jnp.transpose(jnp.broadcast_to(row, (HEAD, tile))).astype(jnp.int32)
            buf[t * tile : (t + 1) * tile, :] = column
        start, last_start = jnp.min(start_row).astype(jnp.int32), jnp.max(start_row).astype(jnp.int32)
        bounds.append((start, jnp.max(end_row).astype(jnp.int32), start == last_start))

    def base_of(t):
        return (bounds[t][0] // ALIGN) * ALIGN

    def blocks_of(t):
        return (bounds[t][1] - base_of(t) + KEY_BLOCK - 1) // KEY_BLOCK

    first_shard = base_of(0) // rows
    limit = base_of(0)
    for t in range(rows // tile):
        limit = jnp.maximum(limit, base_of(t) + blocks_of(t) * KEY_BLOCK)
    last_shard = jnp.minimum((limit + rows - 1) // rows, shards)

    def k_copy(s):
        return pltpu.make_async_copy(
            kv_ref.at[s, pl.ds(0, rows), pl.ds(0, HEAD)],
            k_buf.at[pl.ds(pl.multiple_of(s * rows, rows), rows), :],
            sem.at[s],
        )

    def v_copy(s):
        return pltpu.make_async_copy(
            kv_ref.at[s, pl.ds(0, rows), pl.ds(HEAD, HEAD)],
            v_buf.at[pl.ds(pl.multiple_of(s * rows, rows), rows), pl.ds(0, HEAD)],
            sem.at[shards + s],
        )

    @pl.loop(first_shard, last_shard)
    def _(s):
        k_copy(s).start()
        v_copy(s).start()

    waited = first_shard
    for t in range(rows // tile):
        base = base_of(t)
        q = q_ref[:, t * tile : (t + 1) * tile, :].reshape(heads * tile, HEAD)
        acc[...] = jnp.zeros_like(acc)
        top[...] = jnp.full_like(top, -1e30)
        start, end, single = bounds[t]

        def advance(q, offset, masked, t=t):
            offset = pl.multiple_of(offset, ALIGN)
            keys = k_buf[pl.ds(offset, KEY_BLOCK), :]
            values = v_buf[pl.ds(offset, KEY_BLOCK), :]
            scores = lax.dot_general(q, keys, (((1,), (1,)), ((), ())), preferred_element_type=jnp.float32)
            if masked:
                place = offset + lax.broadcasted_iota(jnp.int32, (heads * tile, KEY_BLOCK), 1)
                reps = KEY_BLOCK // HEAD

                def spread(buf):
                    one = buf[t * tile : (t + 1) * tile, :]
                    both = jnp.concatenate([one] * heads, axis=0)
                    return jnp.concatenate([both] * reps, axis=1)

                allowed = (place >= spread(start_buf)) & (place < spread(end_buf))
                scores = jnp.where(allowed, scores, -1e30)
            old = top[...]
            new = jnp.maximum(old, jnp.max(scores, axis=1, keepdims=True))
            shift = jnp.concatenate([new * LOG2_SCALE] * (KEY_BLOCK // HEAD), axis=1)
            weights = jnp.exp2(scores * LOG2_SCALE - shift)
            if masked:
                weights = jnp.where(allowed, weights, 0.0)
            rescale = jnp.exp2((old - new) * LOG2_SCALE)
            part = jnp.dot(weights.astype(jnp.bfloat16), values, preferred_element_type=jnp.float32)
            acc[...] = acc[...] * jnp.concatenate([rescale, rescale], axis=1) + part
            top[...] = new

        def step(b, waited):
            offset = base + b * KEY_BLOCK
            need = jnp.minimum((offset + KEY_BLOCK + rows - 1) // rows, shards)

            @pl.loop(waited, need)
            def _(s):
                k_copy(s).wait()
                v_copy(s).wait()

            inside = single & (offset >= start) & (offset + KEY_BLOCK <= end)

            @pl.when(inside)
            def _():
                advance(q, offset, False)

            @pl.when(jnp.logical_not(inside))
            def _():
                advance(q, offset, True)

            return jnp.maximum(waited, need)

        waited = lax.fori_loop(0, blocks_of(t), step, waited)
        result = (acc[:, 0:HEAD] / acc[:, HEAD:]).astype(jnp.bfloat16)
        for head in range(heads):
            out_ref[t * tile : (t + 1) * tile, head * HEAD : (head + 1) * HEAD] = result[head * tile : (head + 1) * tile]

    @pl.loop(waited, last_shard)
    def _(s):
        k_copy(s).wait()
        v_copy(s).wait()


def layer_norm(stream, gain_vec, bias_vec):
    center = jnp.mean(stream, axis=-1, keepdims=True)
    spread = jnp.mean(jnp.square(stream - center), axis=-1, keepdims=True)
    return (stream - center) * lax.rsqrt(spread + eps_norm) * gain_vec + bias_vec


def attend(queries, key_heads, value_heads, documents, query_gain, key_gain):
    rows = queries.shape[0]
    heads = queries.shape[1] // HEAD
    shards = lax.axis_size("sp")
    cosine, sine = rotary_tables(rows, lax.axis_index("sp") * rows)
    docs = documents.reshape(2, rows // 2)
    sent = pl.pallas_call(
        key_kernel,
        out_shape=jax.ShapeDtypeStruct((rows + 16, 2 * HEAD), jnp.bfloat16),
        in_specs=[VMEM] * 6,
        out_specs=VMEM,
        cost_estimate=pl.CostEstimate(flops=1000000, bytes_accessed=1000000, transcendentals=0),
        name="keys",
    )(key_heads, value_heads, docs, key_gain.reshape(1, HEAD), cosine, sine)
    filled = lax.all_gather(sent, "sp", axis=0, tiled=False)
    query_rot = pl.pallas_call(
        query_kernel,
        out_shape=jax.ShapeDtypeStruct((heads, rows, HEAD), jnp.bfloat16),
        in_specs=[VMEM] * 4,
        out_specs=VMEM,
        cost_estimate=pl.CostEstimate(flops=1000000, bytes_accessed=1000000, transcendentals=0),
        name="queries",
    )(queries, query_gain.reshape(1, HEAD), cosine, sine)
    tile = rows // 2
    return pl.pallas_call(
        functools.partial(attention_kernel, shards, rows, tile),
        out_shape=jax.ShapeDtypeStruct((rows, heads * HEAD), jnp.bfloat16),
        in_specs=[VMEM, VMEM, ANY],
        out_specs=VMEM,
        scratch_shapes=[
            pltpu.VMEM((shards * rows + KEY_BLOCK, HEAD), jnp.bfloat16),
            pltpu.VMEM((shards * rows + KEY_BLOCK, 2 * HEAD), jnp.bfloat16),
            pltpu.VMEM((shards, 16, 2 * HEAD), jnp.bfloat16),
            pltpu.VMEM((rows, HEAD), jnp.int32),
            pltpu.VMEM((rows, HEAD), jnp.int32),
            pltpu.VMEM((heads * tile, 2 * HEAD), jnp.float32),
            pltpu.VMEM((heads * tile, HEAD), jnp.float32),
            pltpu.SemaphoreType.DMA((2 * shards + 1,)),
        ],
        compiler_params=pltpu.CompilerParams(vmem_limit_bytes=56 * 1024 * 1024),
        cost_estimate=pl.CostEstimate(flops=6000000000, bytes_accessed=9000000, transcendentals=11000000),
        name="attention",
    )(query_rot, docs, filled)


def per_device(
    queries,
    key_heads,
    value_heads,
    documents,
    query_gain,
    key_gain,
    out_gain,
    out_proj,
    residual,
    mid_gain,
    mid_bias,
    routes,
    route_weights,
    expert_gate,
    expert_up,
    expert_down,
    final_gain,
    final_bias,
):
    attention = attend(queries, key_heads, value_heads, documents, query_gain, key_gain)
    tp_size = lax.axis_size("tp")
    tiles = attention.reshape(tp_size, attention.shape[0] // tp_size, attention.shape[1])
    arrived = lax.all_to_all(tiles, "tp", split_axis=0, concat_axis=0, tiled=True)
    attention = jnp.transpose(arrived, (1, 0, 2)).reshape(arrived.shape[1], -1)
    attn_float = attention.astype(jnp.float32)
    mean_square = jnp.mean(attn_float * attn_float, axis=1, keepdims=True)
    scaled = (attn_float * out_gain).astype(jnp.bfloat16)
    projected = jnp.dot(scaled, out_proj, preferred_element_type=jnp.float32)
    projected = projected * lax.rsqrt(mean_square + eps_norm)
    middle = layer_norm(
        alpha_mix * residual.astype(jnp.float32) + projected, mid_gain, mid_bias
    ).astype(jnp.bfloat16)
    out_rows = middle.shape[0]
    model_width = middle.shape[1]
    top_count = routes.shape[1]
    local_experts = expert_gate.shape[0]
    sp_size = lax.axis_size("sp")
    tp_size = lax.axis_size("tp")
    expert_total = local_experts * sp_size * tp_size
    capacity = 2 * out_rows * top_count // expert_total
    flat_routes = routes.reshape(-1)
    one_hot = (flat_routes[:, None] == jnp.arange(expert_total, dtype=jnp.int32)[None, :]).astype(
        jnp.int32
    )
    rank_in = jnp.sum((jnp.cumsum(one_hot, axis=0) - one_hot) * one_hot, axis=1)
    target = flat_routes * capacity + rank_in
    outbound = (
        jnp.zeros((expert_total * capacity, model_width), jnp.bfloat16)
        .at[target]
        .set(jnp.repeat(middle, top_count, axis=0))
    )
    arrived = lax.all_to_all(
        outbound.reshape(expert_total, capacity, model_width),
        ("sp", "tp"),
        split_axis=0,
        concat_axis=0,
        tiled=True,
    )
    item_count = arrived.shape[-2]
    grouped_rows = arrived.reshape(-1, local_experts, item_count, model_width)
    gate_part = jnp.einsum(
        "sekd,edf->sekf", grouped_rows, expert_gate, preferred_element_type=jnp.float32
    )
    up_part = jnp.einsum(
        "sekd,edf->sekf", grouped_rows, expert_up, preferred_element_type=jnp.float32
    )
    hidden = (jax.nn.silu(gate_part) * up_part).astype(jnp.bfloat16)
    served = jnp.einsum("sekf,efd->sekd", hidden, expert_down, preferred_element_type=jnp.float32)
    returned = lax.all_to_all(
        served.astype(jnp.bfloat16).reshape(arrived.shape),
        ("sp", "tp"),
        split_axis=0,
        concat_axis=0,
        tiled=True,
    )
    picked = returned.reshape(expert_total * capacity, model_width)[target]
    picked = picked.astype(jnp.float32).reshape(out_rows, top_count, model_width)
    routed = jnp.sum(picked * route_weights[:, :, None], axis=1)
    return layer_norm(
        alpha_mix * middle.astype(jnp.float32) + routed, final_gain, final_bias
    ).astype(jnp.bfloat16)


def solution(mesh):
    both = ("sp", "tp")
    return jax.shard_map(
        per_device,
        mesh=mesh,
        in_specs=(
            P("sp", "tp"),
            P("sp", "tp"),
            P("sp", "tp"),
            P("sp"),
            P(),
            P(),
            P(),
            P(),
            P(both, None),
            P(),
            P(),
            P(both, None),
            P(both, None),
            P(both, None, None),
            P(both, None, None),
            P(both, None, None),
            P(),
            P(),
        ),
        out_specs=P(both, None),
        check_vma=False,
    )
```

```python
import functools
import math

import jax
import jax.numpy as jnp
import numpy as np
from jax import lax
from jax.experimental import pallas as pl
from jax.experimental.pallas import tpu as pltpu
from jax.sharding import PartitionSpec as P

HEAD = 128
GRID = 64
KEY_BLOCK = 1152
ALIGN = 128

eps_norm = 1e-06
alpha_mix = 8.0**0.25
theta_base = 10000.0
LOG2_SCALE = HEAD ** (-0.5) * math.log2(math.e)

ANY = pl.BlockSpec(memory_space=pl.ANY)
VMEM = pl.BlockSpec(memory_space=pltpu.VMEM)


def turn(values, gain, cosine, sine):
    inv_rms = lax.rsqrt(jnp.mean(values * values, axis=-1, keepdims=True) + eps_norm)
    values = values * inv_rms * gain
    swapped = pltpu.roll(values, HEAD // 2, 1)
    return (values * cosine + swapped * sine).astype(jnp.bfloat16)


def attention_kernel(shards, rows, tile, q_ref, docs_ref, kv_ref, out_ref, k_buf, v_buf, d_buf, start_buf, end_buf, acc, top, sem):
    heads = q_ref.shape[0]
    total_keys = shards * rows
    doc_copy = pltpu.make_async_copy(kv_ref.at[:, pl.ds(rows, 16), :], d_buf, sem.at[2 * shards])
    doc_copy.start()
    v_buf[:, HEAD:] = jnp.ones((v_buf.shape[0], HEAD), jnp.bfloat16)
    v_buf[total_keys:, 0:HEAD] = jnp.zeros((KEY_BLOCK, HEAD), jnp.bfloat16)
    doc_copy.wait()
    all_docs = d_buf[:, 0:8, :].astype(jnp.float32).astype(jnp.int32)[:, 0:2, :]
    docs_here = docs_ref[...]
    half = rows // 2

    counts = [
        jnp.sum(jnp.sum((all_docs < d).astype(jnp.float32), axis=(0, 1), keepdims=False)[None, :], axis=1, keepdims=True)
        for d in range(1, 9)
    ]
    counts = [jnp.zeros((1, 1), jnp.float32)] + counts + [jnp.full((1, 1), float(total_keys), jnp.float32)]
    bounds = []
    for t in range(rows // tile):
        per_row = half // tile
        mine = docs_here[t // per_row : t // per_row + 1, (t % per_row) * tile : (t % per_row + 1) * tile]
        start_row = jnp.zeros(mine.shape, jnp.float32)
        end_row = jnp.zeros(mine.shape, jnp.float32)
        for d in range(9):
            start_row = jnp.where(mine == d, counts[d], start_row)
            end_row = jnp.where(mine == d, counts[d + 1], end_row)
        for row, buf in ((start_row, start_buf), (end_row, end_buf)):
            column = jnp.transpose(jnp.broadcast_to(row, (HEAD, tile))).astype(jnp.int32)
            buf[t * tile : (t + 1) * tile, :] = column
        start, last_start = jnp.min(start_row).astype(jnp.int32), jnp.max(start_row).astype(jnp.int32)
        bounds.append((start, jnp.max(end_row).astype(jnp.int32), start == last_start))

    def base_of(t):
        return (bounds[t][0] // ALIGN) * ALIGN

    def blocks_of(t):
        return (bounds[t][1] - base_of(t) + KEY_BLOCK - 1) // KEY_BLOCK

    first_shard = base_of(0) // rows
    limit = base_of(0)
    for t in range(rows // tile):
        limit = jnp.maximum(limit, base_of(t) + blocks_of(t) * KEY_BLOCK)
    last_shard = jnp.minimum((limit + rows - 1) // rows, shards)

    def k_copy(s):
        return pltpu.make_async_copy(
            kv_ref.at[s, pl.ds(0, rows), pl.ds(0, HEAD)],
            k_buf.at[pl.ds(pl.multiple_of(s * rows, rows), rows), :],
            sem.at[s],
        )

    def v_copy(s):
        return pltpu.make_async_copy(
            kv_ref.at[s, pl.ds(0, rows), pl.ds(HEAD, HEAD)],
            v_buf.at[pl.ds(pl.multiple_of(s * rows, rows), rows), pl.ds(0, HEAD)],
            sem.at[shards + s],
        )

    @pl.loop(first_shard, last_shard)
    def _(s):
        k_copy(s).start()
        v_copy(s).start()

    waited = first_shard
    for t in range(rows // tile):
        base = base_of(t)
        q = q_ref[:, t * tile : (t + 1) * tile, :].reshape(heads * tile, HEAD)
        acc[...] = jnp.zeros_like(acc)
        top[...] = jnp.full_like(top, -1e30)
        start, end, single = bounds[t]

        def advance(q, offset, masked, t=t):
            offset = pl.multiple_of(offset, ALIGN)
            keys = k_buf[pl.ds(offset, KEY_BLOCK), :]
            values = v_buf[pl.ds(offset, KEY_BLOCK), :]
            scores = lax.dot_general(q, keys, (((1,), (1,)), ((), ())), preferred_element_type=jnp.float32)
            if masked:
                place = offset + lax.broadcasted_iota(jnp.int32, (heads * tile, KEY_BLOCK), 1)
                reps = KEY_BLOCK // HEAD

                def spread(buf):
                    one = buf[t * tile : (t + 1) * tile, :]
                    both = jnp.concatenate([one] * heads, axis=0)
                    return jnp.concatenate([both] * reps, axis=1)

                allowed = (place >= spread(start_buf)) & (place < spread(end_buf))
                scores = jnp.where(allowed, scores, -1e30)
            old = top[...]
            new = jnp.maximum(old, jnp.max(scores, axis=1, keepdims=True))
            shift = jnp.concatenate([new * LOG2_SCALE] * (KEY_BLOCK // HEAD), axis=1)
            weights = jnp.exp2(scores * LOG2_SCALE - shift)
            if masked:
                weights = jnp.where(allowed, weights, 0.0)
            rescale = jnp.exp2((old - new) * LOG2_SCALE)
            part = jnp.dot(weights.astype(jnp.bfloat16), values, preferred_element_type=jnp.float32)
            acc[...] = acc[...] * jnp.concatenate([rescale, rescale], axis=1) + part
            top[...] = new

        def step(b, waited):
            offset = base + b * KEY_BLOCK
            need = jnp.minimum((offset + KEY_BLOCK + rows - 1) // rows, shards)

            @pl.loop(waited, need)
            def _(s):
                k_copy(s).wait()
                v_copy(s).wait()

            inside = single & (offset >= start) & (offset + KEY_BLOCK <= end)

            @pl.when(inside)
            def _():
                advance(q, offset, False)

            @pl.when(jnp.logical_not(inside))
            def _():
                advance(q, offset, True)

            return jnp.maximum(waited, need)

        waited = lax.fori_loop(0, blocks_of(t), step, waited)
        result = (acc[:, 0:HEAD] / acc[:, HEAD:]).astype(jnp.bfloat16)
        for head in range(heads):
            out_ref[t * tile : (t + 1) * tile, head * HEAD : (head + 1) * HEAD] = result[head * tile : (head + 1) * tile]

    @pl.loop(waited, last_shard)
    def _(s):
        k_copy(s).wait()
        v_copy(s).wait()


NZ, NY, NC, NX = 4, 4, 2, 4
CAP = 4
WIDE = 512
MESH = pl.DeviceIdType.MESH


def table_constants():
    pairs = HEAD // 4
    inv_freq = (theta_base ** (-np.arange(pairs, dtype=np.float32) / np.float32(pairs))).astype(np.float32)
    tables = []
    for count, lane in ((NZ * NY * NC * 8, 0), (GRID, pairs)):
        angle = np.arange(count, dtype=np.float32)[:, None] * inv_freq[None, :]
        cosine = np.zeros((count, HEAD), np.float32)
        sine = np.zeros((count, HEAD), np.float32)
        for start, sign in ((lane, -1.0), (lane + HEAD // 2, 1.0)):
            cosine[:, start : start + pairs] = np.cos(angle.astype(np.float64))
            sine[:, start : start + pairs] = sign * np.sin(angle.astype(np.float64))
        tables += [cosine, sine]
    return tables


PIECES = ((0, 128), (128, 128), (256, 128), (384, 144))


def span(half, part):
    if part is None:
        return PIECES[2 * half][0], PIECES[2 * half][1] + PIECES[2 * half + 1][1]
    return PIECES[2 * half + part]


def gather_events():
    first, second, third, fourth = [], [], [], []
    for half in (0, 1):
        first += [(half, 0, 1, None), (half, 0, -1, None), (half, 1, 0, None), (half, -1, 0, None)]
        second += [(half, 0, 2, 0), (half, 0, 2, 1), (half, 2, 0, 0), (half, 2, 0, 1)]
        third += [(half, i, j, None) for j in (1, -1) for i in (1, -1)]
        fourth += [(half, i, 2, p) for p in (0, 1) for i in (1, -1)]
        fourth += [(half, 2, j, p) for j in (1, -1) for p in (0, 1)]
    last = [(half, 2, 2, p) for p in (0, 1) for half in (0, 1)]
    return first + second + third + fourth + last


EVENTS = gather_events()
EVENT_ID = {e: n for n, e in enumerate(EVENTS)}


def sends_of(event):
    half, i, j, part = event
    out = []
    if i == 0 and j == 0:
        out += [(0, s, (half, 0, s, None)) for s in (1, -1)]
        out += [(1, s, (half, s, 0, None)) for s in (1, -1)]
    elif i == 0:
        if j == 1:
            out.append((0, 1, (half, 0, 2, 0)))
        if j == -1:
            out.append((0, -1, (half, 0, 2, 1)))
        out += [(1, s, (half, s, j, part)) for s in (1, -1)]
    elif i == 1 and part in (None, 0):
        out.append((1, 1, (half, 2, j, 0)))
    elif i == -1 and part in (None, 1):
        out.append((1, -1, (half, 2, j, 1)))
    return out


SEND_TOTAL = sum(len(sends_of(e)) for e in EVENTS + [(0, 0, 0, None), (1, 0, 0, None)])


def gather_kernel(
    query_ref, key_ref, value_ref, docs_ref, qgain_ref, kgain_ref, rowc_ref, rows_ref, colc_ref, cols_ref,
    kv_ref, q_ref, own, send_sem, recv_sem, pair_send, pair_recv, local_sem,
):
    sp, tp = lax.axis_index("sp"), lax.axis_index("tp")
    core = sp % NC
    y = (sp // NC) % NY
    z = sp // (NC * NY)
    rows = key_ref.shape[0]

    def shard_at(dz, dy):
        return ((z + dz + 2 * NZ) % NZ) * (NY * NC) + ((y + dy + 2 * NY) % NY) * NC + core

    partner = sp + 1 - 2 * core
    barrier = pltpu.get_barrier_semaphore()
    for dz, dy in ((0, 1), (0, -1), (1, 0), (-1, 0)):
        pl.semaphore_signal(barrier, inc=1, device_id=(shard_at(dz, dy), tp), device_id_type=MESH)
    pl.semaphore_signal(barrier, inc=1, device_id=(partner, tp), device_id_type=MESH)

    def table(row_ref, col_ref):
        near = row_ref[pl.ds(pl.multiple_of(sp * 8, 8), 8), :]
        return jnp.concatenate([col_ref[...] + near[n : n + 1, :] for n in range(8)], axis=0)

    cosine, sine = table(rowc_ref, colc_ref), table(rows_ref, cols_ref)
    own[0:rows, 0:HEAD] = turn(key_ref[...].astype(jnp.float32), kgain_ref[...], cosine, sine)
    own[0:rows, HEAD:] = value_ref[...]
    docs = docs_ref[...].astype(jnp.float32)
    padded = jnp.concatenate([docs, jnp.zeros((16 - docs.shape[0], docs.shape[1]), jnp.float32)], axis=0)
    own[rows:, :] = padded.astype(jnp.bfloat16)
    pl.semaphore_wait(barrier, 5)

    started = []
    counter = [0]

    def place(event):
        half, i, j, part = event
        return (-i, -j) if half == 0 else (-j, -i)

    def pass_on(event, source):
        for axis, step, target in sends_of(event):
            half, i, j, part = target
            along_y = (axis == 0) == (half == 0)
            start, size = span(half, part)
            shard = shard_at(*place(event))
            dst = kv_ref.at[shard, pl.ds(start, size), :]
            src = own.at[pl.ds(start, size), :] if source is None else dst
            copy = pltpu.make_async_remote_copy(
                src_ref=src,
                dst_ref=dst,
                send_sem=send_sem.at[counter[0]],
                recv_sem=recv_sem.at[EVENT_ID[target]],
                device_id=(shard_at(0, step) if along_y else shard_at(step, 0), tp),
                device_id_type=MESH,
            )
            counter[0] += 1
            copy.start()
            started.append(copy)

    def to_partner(shard, start, size, src, number):
        copy = pltpu.make_async_remote_copy(
            src_ref=src,
            dst_ref=kv_ref.at[shard, pl.ds(start, size), :],
            send_sem=pair_send.at[number],
            recv_sem=pair_recv.at[0],
            device_id=(partner, tp),
            device_id_type=MESH,
        )
        copy.start()
        started.append(copy)

    for half in (0, 1):
        pass_on((half, 0, 0, None), None)
    to_partner(sp, 0, rows + 16, own, len(EVENTS))
    keep = pltpu.make_async_copy(own, kv_ref.at[sp], local_sem.at[0])
    keep.start()
    for head in range(q_ref.shape[0]):
        q_ref[head] = turn(
            query_ref[:, head * HEAD : (head + 1) * HEAD].astype(jnp.float32), qgain_ref[...], cosine, sine
        )
    for number, event in enumerate(EVENTS):
        half, i, j, part = event
        shard = shard_at(*place(event))
        start, size = span(half, part)
        here = kv_ref.at[shard, pl.ds(start, size), :]
        pltpu.make_async_copy(here, here, recv_sem.at[number]).wait()
        pass_on(event, here)
        to_partner(shard, start, size, here, number)
    every = kv_ref.at[pl.ds(0, NZ * NY), :, :]
    pltpu.make_async_copy(every, every, pair_recv.at[0]).wait()
    keep.wait()
    for copy in started:
        copy.wait_send()


def norm_rows(stream, gain, bias):
    center = jnp.mean(stream, axis=-1, keepdims=True)
    spread = jnp.mean(jnp.square(stream - center), axis=-1, keepdims=True)
    return (stream - center) * lax.rsqrt(spread + eps_norm) * gain + bias


def expert_kernel(
    att_ref, res_ref, routes_ref, weights_ref, ogain_ref, mgain_ref, mbias_ref, fgain_ref, fbias_ref,
    proj_hbm, gate_hbm, up_hbm, down_hbm,
    out_ref,
    att_buf, proj, gate, up, down, stream, mid, sent, got, served, back, picked, xs,
    load_sem, att_send, att_recv, go_send, go_recv, ret_send, ret_recv,
):
    sp, tp = lax.axis_index("sp"), lax.axis_index("tp")
    core = sp % NC
    y = (sp // NC) % NY
    z = sp // (NC * NY)
    tokens = res_ref.shape[0]
    width = res_ref.shape[1]
    chunks = width // WIDE
    block = CAP * chunks
    groups = 4
    per_group = NZ * NY * NC * NX // groups
    group_rows = per_group * block

    loads = [
        pltpu.make_async_copy(src, dst, load_sem.at[n])
        for n, (src, dst) in enumerate(((proj_hbm, proj), (gate_hbm.at[0], gate), (up_hbm.at[0], up), (down_hbm.at[0], down)))
    ]
    for load in loads:
        load.start()

    def steps(g, r):
        dx, dy, dc = r // (NY * NC), (r // NC) % NY, r % NC
        return dx, dy, (g + 8 - dx - dy) % NZ, dc

    def device_at(g, r, sign):
        dx, dy, dz, dc = steps(g, r)
        new_z = (z + NZ + sign * dz) % NZ
        new_y = (y + NY + sign * dy) % NY
        new_c = (core + dc) % NC
        new_x = (tp + NX + sign * dx) % NX
        return (new_z * (NY * NC) + new_y * NC + new_c, new_x)

    barrier = pltpu.get_barrier_semaphore()
    for g in range(groups):

        @pl.loop(1 if g == 0 else 0, per_group)
        def _(r, g=g):
            pl.semaphore_signal(barrier, inc=1, device_id=device_at(g, r, 1), device_id_type=MESH)

    named = routes_ref[...]
    expert_lane = lax.broadcasted_iota(jnp.int32, (tokens, 128), 1)
    hot = [(named[:, k : k + 1] == expert_lane).astype(jnp.float32) for k in (0, 1)]
    earlier = (
        lax.broadcasted_iota(jnp.int32, (tokens, tokens), 1) < lax.broadcasted_iota(jnp.int32, (tokens, tokens), 0)
    ).astype(jnp.bfloat16)
    counted = jnp.dot(earlier, (hot[0] + hot[1]).astype(jnp.bfloat16), preferred_element_type=jnp.float32)
    slot_column, slot_row = [], []
    for k in (0, 1):
        rank = jnp.sum(hot[k] * counted, axis=1, keepdims=True).astype(jnp.int32)
        e = named[:, k : k + 1]
        dx = ((e & 3) + NX - tp) & 3
        dc = (((e >> 2) & 1) + core) & 1
        dy = (((e >> 3) & 3) + NY - y) & 3
        dz = ((e >> 5) + NZ - z) & 3
        place = ((dx + dy + dz) & 3) * per_group + dx * (NY * NC) + dy * NC + dc
        column = place * block + rank
        slot_column.append(column)
        turned = jnp.transpose(jnp.broadcast_to(column.astype(jnp.float32), (tokens, 128)))
        row = turned[0:1, :].astype(jnp.int32)
        slot_row.append(jnp.concatenate([row + CAP * c for c in range(chunks)], axis=1))

    pl.semaphore_wait(barrier, NZ * NY * NC * NX - 1)

    copies = []
    for j in range(1, NX):
        to = (tp + j) % NX
        copy = pltpu.make_async_remote_copy(
            src_ref=att_ref.at[pl.ds(pl.multiple_of(to * tokens, tokens), tokens), :],
            dst_ref=att_buf.at[j],
            send_sem=att_send.at[j],
            recv_sem=att_recv.at[j],
            device_id=(sp, to),
            device_id_type=MESH,
        )
        copy.start()
        copies.append(copy)

    loads[0].wait()
    squares = jnp.zeros((tokens, 1), jnp.float32)
    local = att_ref.shape[1]
    for j in range(NX):
        source = (tp + NX - j) % NX
        if j == 0:
            part = att_ref[pl.ds(pl.multiple_of(tp * tokens, tokens), tokens), :]
        else:
            copies[j - 1].wait_recv()
            part = att_buf[j]
        part = part.astype(jnp.float32)
        squares = squares + jnp.sum(part * part, axis=1, keepdims=True)
        scaled = (part * ogain_ref[pl.ds(source, 1), :]).astype(jnp.bfloat16)
        product = jnp.dot(
            scaled, proj[pl.ds(pl.multiple_of(source * local, local), local), :], preferred_element_type=jnp.float32
        )
        if j == 0:
            stream[...] = product
        else:
            stream[...] += product
    inv_rms = lax.rsqrt(squares / (NX * local) + eps_norm)

    step_rows = 16
    for n in range(tokens // step_rows):
        part = slice(n * step_rows, (n + 1) * step_rows)
        value = alpha_mix * res_ref[part, :].astype(jnp.float32) + stream[part, :] * inv_rms[part, :]
        value = norm_rows(value, mgain_ref[...], mbias_ref[...]).astype(jnp.bfloat16)
        for c in range(chunks):
            mid[c * tokens + n * step_rows : c * tokens + (n + 1) * step_rows, :] = value[:, c * WIDE : (c + 1) * WIDE]

    def row_iota(g):
        return lax.broadcasted_iota(jnp.int32, (group_rows, chunks * tokens), 0) + g * group_rows

    for g in range(groups):
        rows = row_iota(g)
        choose = ((rows == slot_row[0]) | (rows == slot_row[1])).astype(jnp.float32).astype(jnp.bfloat16)
        sent[g * group_rows : (g + 1) * group_rows, :] = jnp.dot(
            choose, mid[...], preferred_element_type=jnp.float32
        ).astype(jnp.bfloat16)

        @pl.loop(1 if g == 0 else 0, per_group)
        def _(r, g=g):
            at = pl.ds(pl.multiple_of((g * per_group + r) * block, block), block)
            pltpu.make_async_remote_copy(
                src_ref=sent.at[at, :],
                dst_ref=got.at[at, :],
                send_sem=go_send.at[g],
                recv_sem=go_recv.at[g],
                device_id=device_at(g, r, 1),
                device_id_type=MESH,
            ).start()

    got[0:block, :] = sent[0:block, :]
    for load in loads[1:]:
        load.wait()

    def whole(ref, g):
        first = block if g == 0 else 0
        return ref.at[pl.ds(g * group_rows + first, group_rows - first), :]

    sub = 256
    ii = lax.broadcasted_iota(jnp.int32, (sub, sub), 0)
    jj = lax.broadcasted_iota(jnp.int32, (sub, sub), 1)
    per_chunk = sub // chunks

    def spot(i):
        return ((i % per_chunk) // CAP) * block + (i // per_chunk) * CAP + i % CAP

    collect = (jj == spot(ii)).astype(jnp.float32).astype(jnp.bfloat16)
    scatter = (ii == spot(jj)).astype(jnp.float32).astype(jnp.bfloat16)
    for g in range(groups):
        pltpu.make_async_copy(whole(got, g), whole(got, g), go_recv.at[g]).wait()
        for s in range(group_rows // sub):
            ordered = jnp.dot(
                collect, got[g * group_rows + s * sub : g * group_rows + (s + 1) * sub, :], preferred_element_type=jnp.float32
            ).astype(jnp.bfloat16)
            for c in range(chunks):
                xs[s * per_chunk : (s + 1) * per_chunk, c * WIDE : (c + 1) * WIDE] = ordered[
                    c * per_chunk : (c + 1) * per_chunk, :
                ]
        x = xs[...]
        gate_part = jnp.dot(x, gate[...], preferred_element_type=jnp.float32)
        up_part = jnp.dot(x, up[...], preferred_element_type=jnp.float32)
        hidden = (gate_part / (1.0 + jnp.exp(-gate_part)) * up_part).astype(jnp.bfloat16)
        result = jnp.dot(hidden, down[...], preferred_element_type=jnp.float32).astype(jnp.bfloat16)
        for s in range(group_rows // sub):
            stacked = jnp.concatenate(
                [result[s * per_chunk : (s + 1) * per_chunk, c * WIDE : (c + 1) * WIDE] for c in range(chunks)], axis=0
            )
            served[g * group_rows + s * sub : g * group_rows + (s + 1) * sub, :] = jnp.dot(
                scatter, stacked, preferred_element_type=jnp.float32
            ).astype(jnp.bfloat16)

        @pl.loop(1 if g == 0 else 0, per_group)
        def _(r, g=g):
            at = pl.ds(pl.multiple_of((g * per_group + r) * block, block), block)
            pltpu.make_async_remote_copy(
                src_ref=served.at[at, :],
                dst_ref=back.at[at, :],
                send_sem=ret_send.at[g],
                recv_sem=ret_recv.at[g],
                device_id=device_at(g, r, -1),
                device_id_type=MESH,
            ).start()

    back[0:block, :] = served[0:block, :]

    for g in range(groups):
        pltpu.make_async_copy(whole(back, g), whole(back, g), ret_recv.at[g]).wait()
        lanes = lax.broadcasted_iota(jnp.int32, (tokens, group_rows), 1) + g * group_rows
        arrived = back[g * group_rows : (g + 1) * group_rows, :]
        for c in range(chunks):
            total = jnp.zeros((tokens, WIDE), jnp.float32)
            for k in (0, 1):
                choose = (lanes == slot_column[k] + CAP * c).astype(jnp.float32).astype(jnp.bfloat16)
                total = total + weights_ref[:, k : k + 1] * jnp.dot(choose, arrived, preferred_element_type=jnp.float32)
            if g == 0:
                picked[:, c * WIDE : (c + 1) * WIDE] = total
            else:
                picked[:, c * WIDE : (c + 1) * WIDE] += total

    for n in range(tokens // step_rows):
        part = slice(n * step_rows, (n + 1) * step_rows)
        value = jnp.concatenate(
            [mid[c * tokens + n * step_rows : c * tokens + (n + 1) * step_rows, :] for c in range(chunks)], axis=1
        )
        value = alpha_mix * value.astype(jnp.float32) + picked[part, :]
        out_ref[part, :] = norm_rows(value, fgain_ref[...], fbias_ref[...]).astype(jnp.bfloat16)

    for copy in copies:
        copy.wait_send()
    for g in range(groups):
        pltpu.make_async_copy(whole(sent, g), whole(sent, g), go_send.at[g]).wait()
        pltpu.make_async_copy(whole(served, g), whole(served, g), ret_send.at[g]).wait()


def per_device(
    queries, key_heads, value_heads, documents, query_gain, key_gain, out_gain, out_proj, residual, mid_gain, mid_bias,
    routes, route_weights, expert_gate, expert_up, expert_down, final_gain, final_bias,
):
    rows = queries.shape[0]
    heads = queries.shape[1] // HEAD
    shards = NZ * NY * NC
    docs = documents.reshape(2, rows // 2)
    filled, query_rot = pl.pallas_call(
        gather_kernel,
        out_shape=(
            jax.ShapeDtypeStruct((shards, rows + 16, 2 * HEAD), jnp.bfloat16),
            jax.ShapeDtypeStruct((heads, rows, HEAD), jnp.bfloat16),
        ),
        in_specs=[VMEM] * 10,
        out_specs=(ANY, VMEM),
        scratch_shapes=[
            pltpu.VMEM((rows + 16, 2 * HEAD), jnp.bfloat16),
            pltpu.SemaphoreType.DMA((SEND_TOTAL,)),
            pltpu.SemaphoreType.DMA((len(EVENTS),)),
            pltpu.SemaphoreType.DMA((len(EVENTS) + 1,)),
            pltpu.SemaphoreType.DMA((1,)),
            pltpu.SemaphoreType.DMA((1,)),
        ],
        compiler_params=pltpu.CompilerParams(collective_id=0, has_side_effects=True),
        name="gather",
    )(
        queries, key_heads, value_heads, docs, query_gain.reshape(1, HEAD), key_gain.reshape(1, HEAD),
        *[jnp.asarray(t) for t in table_constants()],
    )
    tile = rows // 2
    attention = pl.pallas_call(
        functools.partial(attention_kernel, shards, rows, tile),
        out_shape=jax.ShapeDtypeStruct((rows, heads * HEAD), jnp.bfloat16),
        in_specs=[VMEM, VMEM, ANY],
        out_specs=VMEM,
        scratch_shapes=[
            pltpu.VMEM((shards * rows + KEY_BLOCK, HEAD), jnp.bfloat16),
            pltpu.VMEM((shards * rows + KEY_BLOCK, 2 * HEAD), jnp.bfloat16),
            pltpu.VMEM((shards, 16, 2 * HEAD), jnp.bfloat16),
            pltpu.VMEM((rows, HEAD), jnp.int32),
            pltpu.VMEM((rows, HEAD), jnp.int32),
            pltpu.VMEM((heads * tile, 2 * HEAD), jnp.float32),
            pltpu.VMEM((heads * tile, HEAD), jnp.float32),
            pltpu.SemaphoreType.DMA((2 * shards + 1,)),
        ],
        compiler_params=pltpu.CompilerParams(vmem_limit_bytes=56 * 1024 * 1024),
        name="attention",
    )(query_rot, docs, filled)
    tokens, width = residual.shape
    hidden = expert_gate.shape[2]
    slots = NZ * NY * NC * NX * CAP * (width // WIDE)
    vec = lambda v: v.reshape(1, -1)
    return pl.pallas_call(
        expert_kernel,
        out_shape=jax.ShapeDtypeStruct((tokens, width), jnp.bfloat16),
        in_specs=[VMEM] * 9 + [ANY] * 4,
        out_specs=VMEM,
        scratch_shapes=[
            pltpu.VMEM((NX, tokens, heads * HEAD), jnp.bfloat16),
            pltpu.VMEM(out_proj.shape, jnp.bfloat16),
            pltpu.VMEM((width, hidden), jnp.bfloat16),
            pltpu.VMEM((width, hidden), jnp.bfloat16),
            pltpu.VMEM((hidden, width), jnp.bfloat16),
            pltpu.VMEM((tokens, width), jnp.float32),
            pltpu.VMEM((width // WIDE * tokens, WIDE), jnp.bfloat16),
            pltpu.VMEM((slots, WIDE), jnp.bfloat16),
            pltpu.VMEM((slots, WIDE), jnp.bfloat16),
            pltpu.VMEM((slots, WIDE), jnp.bfloat16),
            pltpu.VMEM((slots, WIDE), jnp.bfloat16),
            pltpu.VMEM((tokens, width), jnp.float32),
            pltpu.VMEM((tokens, width), jnp.bfloat16),
            pltpu.SemaphoreType.DMA((4,)),
            pltpu.SemaphoreType.DMA((NX,)),
            pltpu.SemaphoreType.DMA((NX,)),
            pltpu.SemaphoreType.DMA((4,)),
            pltpu.SemaphoreType.DMA((4,)),
            pltpu.SemaphoreType.DMA((4,)),
            pltpu.SemaphoreType.DMA((4,)),
        ],
        compiler_params=pltpu.CompilerParams(
            collective_id=1, has_side_effects=True, vmem_limit_bytes=56 * 1024 * 1024
        ),
        name="experts",
    )(
        attention, residual, routes, route_weights, out_gain.reshape(NX, -1), vec(mid_gain), vec(mid_bias),
        vec(final_gain), vec(final_bias), out_proj, expert_gate, expert_up, expert_down,
    )


def solution(mesh):
    both = ("sp", "tp")
    return jax.shard_map(
        per_device,
        mesh=mesh,
        in_specs=(
            P("sp", "tp"),
            P("sp", "tp"),
            P("sp", "tp"),
            P("sp"),
            P(),
            P(),
            P(),
            P(),
            P(both, None),
            P(),
            P(),
            P(both, None),
            P(both, None),
            P(both, None, None),
            P(both, None, None),
            P(both, None, None),
            P(),
            P(),
        ),
        out_specs=P(both, None),
        check_vma=False,
    )
```

```python
import functools
import math

import jax
import jax.numpy as jnp
import numpy as np
from jax import lax
from jax.experimental import pallas as pl
from jax.experimental.pallas import tpu as pltpu
from jax.sharding import PartitionSpec as P

HEAD = 128
GRID = 64

eps_norm = 1e-06
alpha_mix = 8.0**0.25
theta_base = 10000.0
LOG2_SCALE = HEAD ** (-0.5) * math.log2(math.e)

ANY = pl.BlockSpec(memory_space=pl.ANY)
VMEM = pl.BlockSpec(memory_space=pltpu.VMEM)


def turn(values, gain, cosine, sine):
    inv_rms = lax.rsqrt(jnp.mean(values * values, axis=-1, keepdims=True) + eps_norm)
    values = values * inv_rms * gain
    swapped = pltpu.roll(values, HEAD // 2, 1)
    return (values * cosine + swapped * sine).astype(jnp.bfloat16)


NZ, NY, NC, NX = 4, 4, 2, 4
CAP = 4
WIDE = 512
MESH = pl.DeviceIdType.MESH


def table_constants():
    pairs = HEAD // 4
    inv_freq = (theta_base ** (-np.arange(pairs, dtype=np.float32) / np.float32(pairs))).astype(np.float32)
    tables = []
    for count, lane in ((NZ * NY * NC * 8, 0), (GRID, pairs)):
        angle = np.arange(count, dtype=np.float32)[:, None] * inv_freq[None, :]
        cosine = np.zeros((count, HEAD), np.float32)
        sine = np.zeros((count, HEAD), np.float32)
        for start, sign in ((lane, -1.0), (lane + HEAD // 2, 1.0)):
            cosine[:, start : start + pairs] = np.cos(angle.astype(np.float64))
            sine[:, start : start + pairs] = sign * np.sin(angle.astype(np.float64))
        tables += [cosine, sine]
    return tables


DOC_ROWS = 16
HALF_ROWS = HEAD + DOC_ROWS + HEAD
PART_ROWS = ((0, HEAD + DOC_ROWS), (HEAD + DOC_ROWS, HEAD))
SAME_DOC = 32768.0


def span(part):
    return (0, HALF_ROWS) if part is None else PART_ROWS[part]


def gather_events():
    first, second, third, fourth = [], [], [], []
    for half in (0, 1):
        first += [(half, 0, 1, None), (half, 0, -1, None), (half, 1, 0, None), (half, -1, 0, None)]
        second += [(half, 0, 2, 0), (half, 0, 2, 1), (half, 2, 0, 0), (half, 2, 0, 1)]
        third += [(half, i, j, None) for j in (1, -1) for i in (1, -1)]
        fourth += [(half, i, 2, p) for p in (0, 1) for i in (1, -1)]
        fourth += [(half, 2, j, p) for j in (1, -1) for p in (0, 1)]
    last = [(half, 2, 2, p) for p in (0, 1) for half in (0, 1)]
    return first + second + third + fourth + last


EVENTS = gather_events()
EVENT_ID = {e: n for n, e in enumerate(EVENTS)}
UNITS = [(0, (0, 0)), (1, (0, 0)), (0, (0, -1)), (0, (0, 1)), (0, (-1, 0)), (0, (1, 0)), (1, (-1, 0)), (1, (1, 0)), (1, (0, -1)), (1, (0, 1)), (0, (0, 2)), (0, (-1, -1)), (0, (1, -1)), (1, (-1, -1)), (1, (-1, 1)), (0, (-1, 1)), (0, (1, 1)), (0, (2, 0)), (1, (1, -1)), (1, (1, 1)), (1, (2, 0)), (1, (0, 2)), (1, (-1, 2)), (0, (1, 2)), (0, (-1, 2)), (1, (1, 2)), (0, (2, -1)), (1, (2, 1)), (0, (2, 1)), (1, (2, -1)), (0, (2, 2)), (1, (2, 2))]
GAPS = [[], [0, 1, 2, 3], [4, 5, 6, 7], [9, 8], [16, 17], [20, 21, 18, 19], [11, 10, 22, 23], [13, 12, 15, 14], [27, 26, 37, 36, 25, 39, 24], [38, 29, 35, 28, 34], [31, 33, 30, 32, 42], [40, 43], [41], [], [], []]
UNIT_ID = {unit: n for n, unit in enumerate(UNITS)}


def sends_of(event):
    half, i, j, part = event
    out = []
    if i == 0 and j == 0:
        out += [(0, s, (half, 0, s, None)) for s in (1, -1)]
        out += [(1, s, (half, s, 0, None)) for s in (1, -1)]
    elif i == 0:
        if j == 1:
            out.append((0, 1, (half, 0, 2, 0)))
        if j == -1:
            out.append((0, -1, (half, 0, 2, 1)))
        out += [(1, s, (half, s, j, part)) for s in (1, -1)]
    elif i == 1 and part in (None, 0):
        out.append((1, 1, (half, 2, j, 0)))
    elif i == -1 and part in (None, 1):
        out.append((1, -1, (half, 2, j, 1)))
    return out


def unit_of(event):
    half, i, j, part = event
    wrap = lambda v: (v + 1) % 4 - 1
    return UNIT_ID[(half, (wrap(-i), wrap(-j)) if half == 0 else (wrap(-j), wrap(-i)))]


OWN = ((0, 0, 0, None), (1, 0, 0, None))
SENDS = [(e, axis, step, target) for e in list(OWN) + EVENTS for axis, step, target in sends_of(e)]


def attention_kernel(
    query_ref, key_ref, value_ref, docs_ref, qgain_ref, kgain_ref, rowc_ref, rows_ref, colc_ref, cols_ref,
    out_ref,
    slots, queries, acc, top, low, send_sem, recv_sem, pair_send, pair_recv,
):
    sp, tp = lax.axis_index("sp"), lax.axis_index("tp")
    core = sp % NC
    y = (sp // NC) % NY
    z = sp // (NC * NY)
    rows = key_ref.shape[0]
    half_rows = rows // 2
    heads = query_ref.shape[1] // HEAD
    partner = sp + 1 - 2 * core
    near = {}
    for step in (1, -1):
        near[True, step] = z * (NY * NC) + ((y + NY + step) % NY) * NC + core
        near[False, step] = ((z + NZ + step) % NZ) * (NY * NC) + y * NC + core

    barrier = pltpu.get_barrier_semaphore()
    for to in list(near.values()) + [partner]:
        pl.semaphore_signal(barrier, inc=1, device_id=(to, tp), device_id_type=MESH)

    def table(row_ref, col_ref):
        mine = row_ref[pl.ds(pl.multiple_of(sp * 8, 8), 8), :]
        return jnp.concatenate([col_ref[...] + mine[n : n + 1, :] for n in range(8)], axis=0)

    cosine, sine = table(rowc_ref, colc_ref), table(rows_ref, cols_ref)
    turned = turn(key_ref[...].astype(jnp.float32), kgain_ref[...], cosine, sine).astype(jnp.float32)
    numbers = lax.broadcasted_iota(jnp.int32, (HEAD, half_rows), 0)
    for h in range(2):
        part = slice(h * half_rows, (h + 1) * half_rows)
        unit = unit_of(OWN[h])
        slots[unit, 0, 0:HEAD, :] = jnp.transpose(turned[part, :]).astype(jnp.bfloat16)
        same = (numbers[0:DOC_ROWS, :] == docs_ref[h : h + 1, :]).astype(jnp.float32)
        slots[unit, 0, HEAD : HEAD + DOC_ROWS, :] = same.astype(jnp.bfloat16)
        for k in range(2):
            slots[unit, 0, HEAD + DOC_ROWS :, k * HEAD : (k + 1) * HEAD] = value_ref[
                h * half_rows + k * HEAD : h * half_rows + (k + 1) * HEAD, :
            ]
    pl.semaphore_wait(barrier, 5)

    def sent_copy(number):
        event, axis, step, target = SENDS[number]
        half = event[0]
        start, size = span(target[3])
        return pltpu.make_async_remote_copy(
            src_ref=slots.at[unit_of(event), 0, pl.ds(start, size), :],
            dst_ref=slots.at[unit_of(target), 0, pl.ds(start, size), :],
            send_sem=send_sem.at[number],
            recv_sem=recv_sem.at[EVENT_ID[target]],
            device_id=(near[(axis == 0) == (half == 0), step], tp),
            device_id_type=MESH,
        )

    def pair_copy(event, number):
        start, size = span(event[3])
        return pltpu.make_async_remote_copy(
            src_ref=slots.at[unit_of(event), 0, pl.ds(start, size), :],
            dst_ref=slots.at[unit_of(event), 1, pl.ds(start, size), :],
            send_sem=pair_send.at[number],
            recv_sem=pair_recv.at[unit_of(event)],
            device_id=(partner, tp),
            device_id_type=MESH,
        )

    def pass_on(event):
        for number, entry in enumerate(SENDS):
            if entry[0] == event:
                sent_copy(number).start()
        pair_copy(event, (list(OWN) + EVENTS).index(event)).start()

    for event in OWN:
        pass_on(event)

    columns = [jnp.transpose((numbers == docs_ref[h : h + 1, :]).astype(jnp.float32)) for h in range(2)]
    same = (jnp.concatenate(columns, axis=0) * SAME_DOC).astype(jnp.bfloat16)
    for head in range(heads):
        queries[head, :, 0:HEAD] = turn(
            query_ref[:, head * HEAD : (head + 1) * HEAD].astype(jnp.float32), qgain_ref[...], cosine, sine
        )
        queries[head, :, HEAD:] = same[:, 0:DOC_ROWS]
    acc[...] = jnp.zeros_like(acc)
    low[...] = jnp.zeros_like(low)
    top[...] = jnp.full_like(top, -1e20)

    def advance(k):
        places = [(2 * k + n, c) for n in range(2) for c in range(2)]
        keys = jnp.concatenate([slots[u, c, 0 : HEAD + DOC_ROWS, :] for u, c in places], axis=1)
        values = jnp.concatenate(
            [slots[u, c, HEAD + DOC_ROWS :, n * HEAD : (n + 1) * HEAD] for u, c in places for n in range(2)], axis=0
        )
        lanes = keys.shape[1] // HEAD
        scores = [jnp.dot(queries[h], keys, preferred_element_type=jnp.float32) for h in range(heads)]
        for h in range(heads):
            old = top[h]
            new = jnp.maximum(old, jnp.max(scores[h], axis=1, keepdims=True))
            rescale = jnp.exp2((old - new) * LOG2_SCALE)
            weights = jnp.exp2((scores[h] - jnp.concatenate([new] * lanes, axis=1)) * LOG2_SCALE)
            sums = weights[:, 0:HEAD]
            for n in range(1, lanes):
                sums = sums + weights[:, n * HEAD : (n + 1) * HEAD]
            low[h] = low[h] * rescale + sums
            top[h] = new
            acc[h] = acc[h] * rescale + jnp.dot(
                weights.astype(jnp.bfloat16), values, preferred_element_type=jnp.float32
            )

    def step(k, carry):
        for n, gap in enumerate(GAPS):

            @pl.when(k == n)
            def _(n=n, gap=gap):
                for number in gap:
                    event = EVENTS[number]
                    start, size = span(event[3])
                    here = slots.at[unit_of(event), 0, pl.ds(start, size), :]
                    pltpu.make_async_copy(here, here, recv_sem.at[number]).wait()
                    pass_on(event)
                for unit in (2 * n, 2 * n + 1):
                    here = slots.at[unit, 1, :, :]
                    pltpu.make_async_copy(here, here, pair_recv.at[unit]).wait()

        advance(k)
        return carry

    lax.fori_loop(0, len(GAPS), step, 0)
    for h in range(heads):
        total = jnp.sum(low[h], axis=1, keepdims=True)
        out_ref[:, h * HEAD : (h + 1) * HEAD] = (acc[h] / total).astype(jnp.bfloat16)
    for number in range(len(SENDS)):
        sent_copy(number).wait_send()
    for number, event in enumerate(list(OWN) + EVENTS):
        pair_copy(event, number).wait_send()


def norm_rows(stream, gain, bias):
    center = jnp.mean(stream, axis=-1, keepdims=True)
    spread = jnp.mean(jnp.square(stream - center), axis=-1, keepdims=True)
    return (stream - center) * lax.rsqrt(spread + eps_norm) * gain + bias


def expert_kernel(
    att_ref, res_ref, routes_ref, weights_ref, ogain_ref, mgain_ref, mbias_ref, fgain_ref, fbias_ref,
    proj_hbm, gate_hbm, up_hbm, down_hbm,
    out_ref,
    att_buf, proj, gate, up, down, stream, mid, sent, got, served, back, picked, xs,
    load_sem, att_send, att_recv, go_send, go_recv, ret_send, ret_recv,
):
    sp, tp = lax.axis_index("sp"), lax.axis_index("tp")
    core = sp % NC
    y = (sp // NC) % NY
    z = sp // (NC * NY)
    tokens = res_ref.shape[0]
    width = res_ref.shape[1]
    chunks = width // WIDE
    block = CAP * chunks
    groups = 4
    per_group = NZ * NY * NC * NX // groups
    group_rows = per_group * block

    loads = [
        pltpu.make_async_copy(src, dst, load_sem.at[n])
        for n, (src, dst) in enumerate(((proj_hbm, proj), (gate_hbm.at[0], gate), (up_hbm.at[0], up), (down_hbm.at[0], down)))
    ]
    for load in loads:
        load.start()

    def steps(g, r):
        dx, dy, dc = r // (NY * NC), (r // NC) % NY, r % NC
        return dx, dy, (g + 8 - dx - dy) % NZ, dc

    def device_at(g, r, sign):
        dx, dy, dz, dc = steps(g, r)
        new_z = (z + NZ + sign * dz) % NZ
        new_y = (y + NY + sign * dy) % NY
        new_c = (core + dc) % NC
        new_x = (tp + NX + sign * dx) % NX
        return (new_z * (NY * NC) + new_y * NC + new_c, new_x)

    barrier = pltpu.get_barrier_semaphore()
    for g in range(groups):

        @pl.loop(1 if g == 0 else 0, per_group)
        def _(r, g=g):
            pl.semaphore_signal(barrier, inc=1, device_id=device_at(g, r, 1), device_id_type=MESH)

    named = routes_ref[...]
    expert_lane = lax.broadcasted_iota(jnp.int32, (tokens, 128), 1)
    hot = [(named[:, k : k + 1] == expert_lane).astype(jnp.float32) for k in (0, 1)]
    earlier = (
        lax.broadcasted_iota(jnp.int32, (tokens, tokens), 1) < lax.broadcasted_iota(jnp.int32, (tokens, tokens), 0)
    ).astype(jnp.bfloat16)
    counted = jnp.dot(earlier, (hot[0] + hot[1]).astype(jnp.bfloat16), preferred_element_type=jnp.float32)
    slot_column, slot_row = [], []
    for k in (0, 1):
        rank = jnp.sum(hot[k] * counted, axis=1, keepdims=True).astype(jnp.int32)
        e = named[:, k : k + 1]
        dx = ((e & 3) + NX - tp) & 3
        dc = (((e >> 2) & 1) + core) & 1
        dy = (((e >> 3) & 3) + NY - y) & 3
        dz = ((e >> 5) + NZ - z) & 3
        place = ((dx + dy + dz) & 3) * per_group + dx * (NY * NC) + dy * NC + dc
        column = place * block + rank
        slot_column.append(column)
        turned = jnp.transpose(jnp.broadcast_to(column.astype(jnp.float32), (tokens, 128)))
        row = turned[0:1, :].astype(jnp.int32)
        slot_row.append(jnp.concatenate([row + CAP * c for c in range(chunks)], axis=1))

    pl.semaphore_wait(barrier, NZ * NY * NC * NX - 1)

    copies = []
    for j in range(1, NX):
        to = (tp + j) % NX
        copy = pltpu.make_async_remote_copy(
            src_ref=att_ref.at[pl.ds(pl.multiple_of(to * tokens, tokens), tokens), :],
            dst_ref=att_buf.at[j],
            send_sem=att_send.at[j],
            recv_sem=att_recv.at[j],
            device_id=(sp, to),
            device_id_type=MESH,
        )
        copy.start()
        copies.append(copy)

    loads[0].wait()
    squares = jnp.zeros((tokens, 1), jnp.float32)
    local = att_ref.shape[1]
    for j in range(NX):
        source = (tp + NX - j) % NX
        if j == 0:
            part = att_ref[pl.ds(pl.multiple_of(tp * tokens, tokens), tokens), :]
        else:
            copies[j - 1].wait_recv()
            part = att_buf[j]
        part = part.astype(jnp.float32)
        squares = squares + jnp.sum(part * part, axis=1, keepdims=True)
        scaled = (part * ogain_ref[pl.ds(source, 1), :]).astype(jnp.bfloat16)
        product = jnp.dot(
            scaled, proj[pl.ds(pl.multiple_of(source * local, local), local), :], preferred_element_type=jnp.float32
        )
        if j == 0:
            stream[...] = product
        else:
            stream[...] += product
    inv_rms = lax.rsqrt(squares / (NX * local) + eps_norm)

    step_rows = 16
    for n in range(tokens // step_rows):
        part = slice(n * step_rows, (n + 1) * step_rows)
        value = alpha_mix * res_ref[part, :].astype(jnp.float32) + stream[part, :] * inv_rms[part, :]
        value = norm_rows(value, mgain_ref[...], mbias_ref[...]).astype(jnp.bfloat16)
        for c in range(chunks):
            mid[c * tokens + n * step_rows : c * tokens + (n + 1) * step_rows, :] = value[:, c * WIDE : (c + 1) * WIDE]

    def row_iota(g):
        return lax.broadcasted_iota(jnp.int32, (group_rows, chunks * tokens), 0) + g * group_rows

    for g in range(groups):
        rows = row_iota(g)
        choose = ((rows == slot_row[0]) | (rows == slot_row[1])).astype(jnp.float32).astype(jnp.bfloat16)
        sent[g * group_rows : (g + 1) * group_rows, :] = jnp.dot(
            choose, mid[...], preferred_element_type=jnp.float32
        ).astype(jnp.bfloat16)

        @pl.loop(1 if g == 0 else 0, per_group)
        def _(r, g=g):
            at = pl.ds(pl.multiple_of((g * per_group + r) * block, block), block)
            pltpu.make_async_remote_copy(
                src_ref=sent.at[at, :],
                dst_ref=got.at[at, :],
                send_sem=go_send.at[g],
                recv_sem=go_recv.at[g],
                device_id=device_at(g, r, 1),
                device_id_type=MESH,
            ).start()

    got[0:block, :] = sent[0:block, :]
    for load in loads[1:]:
        load.wait()

    def whole(ref, g):
        first = block if g == 0 else 0
        return ref.at[pl.ds(g * group_rows + first, group_rows - first), :]

    sub = 256
    ii = lax.broadcasted_iota(jnp.int32, (sub, sub), 0)
    jj = lax.broadcasted_iota(jnp.int32, (sub, sub), 1)
    per_chunk = sub // chunks

    def spot(i):
        return ((i % per_chunk) // CAP) * block + (i // per_chunk) * CAP + i % CAP

    collect = (jj == spot(ii)).astype(jnp.float32).astype(jnp.bfloat16)
    scatter = (ii == spot(jj)).astype(jnp.float32).astype(jnp.bfloat16)
    for g in range(groups):
        pltpu.make_async_copy(whole(got, g), whole(got, g), go_recv.at[g]).wait()
        for s in range(group_rows // sub):
            ordered = jnp.dot(
                collect, got[g * group_rows + s * sub : g * group_rows + (s + 1) * sub, :], preferred_element_type=jnp.float32
            ).astype(jnp.bfloat16)
            for c in range(chunks):
                xs[s * per_chunk : (s + 1) * per_chunk, c * WIDE : (c + 1) * WIDE] = ordered[
                    c * per_chunk : (c + 1) * per_chunk, :
                ]
        x = xs[...]
        gate_part = jnp.dot(x, gate[...], preferred_element_type=jnp.float32)
        up_part = jnp.dot(x, up[...], preferred_element_type=jnp.float32)
        hidden = (gate_part / (1.0 + jnp.exp(-gate_part)) * up_part).astype(jnp.bfloat16)
        result = jnp.dot(hidden, down[...], preferred_element_type=jnp.float32).astype(jnp.bfloat16)
        for s in range(group_rows // sub):
            stacked = jnp.concatenate(
                [result[s * per_chunk : (s + 1) * per_chunk, c * WIDE : (c + 1) * WIDE] for c in range(chunks)], axis=0
            )
            served[g * group_rows + s * sub : g * group_rows + (s + 1) * sub, :] = jnp.dot(
                scatter, stacked, preferred_element_type=jnp.float32
            ).astype(jnp.bfloat16)

        @pl.loop(1 if g == 0 else 0, per_group)
        def _(r, g=g):
            at = pl.ds(pl.multiple_of((g * per_group + r) * block, block), block)
            pltpu.make_async_remote_copy(
                src_ref=served.at[at, :],
                dst_ref=back.at[at, :],
                send_sem=ret_send.at[g],
                recv_sem=ret_recv.at[g],
                device_id=device_at(g, r, -1),
                device_id_type=MESH,
            ).start()

    back[0:block, :] = served[0:block, :]

    for g in range(groups):
        pltpu.make_async_copy(whole(back, g), whole(back, g), ret_recv.at[g]).wait()
        lanes = lax.broadcasted_iota(jnp.int32, (tokens, group_rows), 1) + g * group_rows
        arrived = back[g * group_rows : (g + 1) * group_rows, :]
        for c in range(chunks):
            total = jnp.zeros((tokens, WIDE), jnp.float32)
            for k in (0, 1):
                choose = (lanes == slot_column[k] + CAP * c).astype(jnp.float32).astype(jnp.bfloat16)
                total = total + weights_ref[:, k : k + 1] * jnp.dot(choose, arrived, preferred_element_type=jnp.float32)
            if g == 0:
                picked[:, c * WIDE : (c + 1) * WIDE] = total
            else:
                picked[:, c * WIDE : (c + 1) * WIDE] += total

    for n in range(tokens // step_rows):
        part = slice(n * step_rows, (n + 1) * step_rows)
        value = jnp.concatenate(
            [mid[c * tokens + n * step_rows : c * tokens + (n + 1) * step_rows, :] for c in range(chunks)], axis=1
        )
        value = alpha_mix * value.astype(jnp.float32) + picked[part, :]
        out_ref[part, :] = norm_rows(value, fgain_ref[...], fbias_ref[...]).astype(jnp.bfloat16)

    for copy in copies:
        copy.wait_send()
    for g in range(groups):
        pltpu.make_async_copy(whole(sent, g), whole(sent, g), go_send.at[g]).wait()
        pltpu.make_async_copy(whole(served, g), whole(served, g), ret_send.at[g]).wait()


def per_device(
    queries, key_heads, value_heads, documents, query_gain, key_gain, out_gain, out_proj, residual, mid_gain, mid_bias,
    routes, route_weights, expert_gate, expert_up, expert_down, final_gain, final_bias,
):
    rows = queries.shape[0]
    heads = queries.shape[1] // HEAD
    docs = documents.reshape(2, rows // 2)
    attention = pl.pallas_call(
        attention_kernel,
        out_shape=jax.ShapeDtypeStruct((rows, heads * HEAD), jnp.bfloat16),
        in_specs=[VMEM] * 10,
        out_specs=VMEM,
        scratch_shapes=[
            pltpu.VMEM((len(UNITS), NC, HALF_ROWS, 2 * HEAD), jnp.bfloat16),
            pltpu.VMEM((heads, rows, HEAD + DOC_ROWS), jnp.bfloat16),
            pltpu.VMEM((heads, rows, HEAD), jnp.float32),
            pltpu.VMEM((heads, rows, HEAD), jnp.float32),
            pltpu.VMEM((heads, rows, HEAD), jnp.float32),
            pltpu.SemaphoreType.DMA((len(SENDS),)),
            pltpu.SemaphoreType.DMA((len(EVENTS),)),
            pltpu.SemaphoreType.DMA((len(EVENTS) + 2,)),
            pltpu.SemaphoreType.DMA((len(UNITS),)),
        ],
        compiler_params=pltpu.CompilerParams(
            collective_id=0, has_side_effects=True, vmem_limit_bytes=48 * 1024 * 1024
        ),
        name="attention",
    )(
        queries, key_heads, value_heads, docs, query_gain.reshape(1, HEAD), key_gain.reshape(1, HEAD),
        *[jnp.asarray(t) for t in table_constants()],
    )
    tokens, width = residual.shape
    hidden = expert_gate.shape[2]
    slots = NZ * NY * NC * NX * CAP * (width // WIDE)
    vec = lambda v: v.reshape(1, -1)
    return pl.pallas_call(
        expert_kernel,
        out_shape=jax.ShapeDtypeStruct((tokens, width), jnp.bfloat16),
        in_specs=[VMEM] * 9 + [ANY] * 4,
        out_specs=VMEM,
        scratch_shapes=[
            pltpu.VMEM((NX, tokens, heads * HEAD), jnp.bfloat16),
            pltpu.VMEM(out_proj.shape, jnp.bfloat16),
            pltpu.VMEM((width, hidden), jnp.bfloat16),
            pltpu.VMEM((width, hidden), jnp.bfloat16),
            pltpu.VMEM((hidden, width), jnp.bfloat16),
            pltpu.VMEM((tokens, width), jnp.float32),
            pltpu.VMEM((width // WIDE * tokens, WIDE), jnp.bfloat16),
            pltpu.VMEM((slots, WIDE), jnp.bfloat16),
            pltpu.VMEM((slots, WIDE), jnp.bfloat16),
            pltpu.VMEM((slots, WIDE), jnp.bfloat16),
            pltpu.VMEM((slots, WIDE), jnp.bfloat16),
            pltpu.VMEM((tokens, width), jnp.float32),
            pltpu.VMEM((tokens, width), jnp.bfloat16),
            pltpu.SemaphoreType.DMA((4,)),
            pltpu.SemaphoreType.DMA((NX,)),
            pltpu.SemaphoreType.DMA((NX,)),
            pltpu.SemaphoreType.DMA((4,)),
            pltpu.SemaphoreType.DMA((4,)),
            pltpu.SemaphoreType.DMA((4,)),
            pltpu.SemaphoreType.DMA((4,)),
        ],
        compiler_params=pltpu.CompilerParams(
            collective_id=1, has_side_effects=True, vmem_limit_bytes=56 * 1024 * 1024
        ),
        name="experts",
    )(
        attention, residual, routes, route_weights, out_gain.reshape(NX, -1), vec(mid_gain), vec(mid_bias),
        vec(final_gain), vec(final_bias), out_proj, expert_gate, expert_up, expert_down,
    )


def solution(mesh):
    both = ("sp", "tp")
    return jax.shard_map(
        per_device,
        mesh=mesh,
        in_specs=(
            P("sp", "tp"),
            P("sp", "tp"),
            P("sp", "tp"),
            P("sp"),
            P(),
            P(),
            P(),
            P(),
            P(both, None),
            P(),
            P(),
            P(both, None),
            P(both, None),
            P(both, None, None),
            P(both, None, None),
            P(both, None, None),
            P(),
            P(),
        ),
        out_specs=P(both, None),
        check_vma=False,
    )
```

```python
import functools
import math

import jax
import jax.numpy as jnp
import numpy as np
from jax import lax
from jax.experimental import pallas as pl
from jax.experimental.pallas import tpu as pltpu
from jax.sharding import PartitionSpec as P

HEAD = 128
GRID = 64

eps_norm = 1e-06
alpha_mix = 8.0**0.25
theta_base = 10000.0
LOG2_SCALE = HEAD ** (-0.5) * math.log2(math.e)

ANY = pl.BlockSpec(memory_space=pl.ANY)
VMEM = pl.BlockSpec(memory_space=pltpu.VMEM)


def turn(values, gain, cosine, sine):
    inv_rms = lax.rsqrt(jnp.mean(values * values, axis=-1, keepdims=True) + eps_norm)
    values = values * inv_rms * gain
    swapped = pltpu.roll(values, HEAD // 2, 1)
    return (values * cosine + swapped * sine).astype(jnp.bfloat16)


NZ, NY, NC, NX = 4, 4, 2, 4
CAP = 4
WIDE = 512
MESH = pl.DeviceIdType.MESH


def table_constants():
    pairs = HEAD // 4
    inv_freq = (theta_base ** (-np.arange(pairs, dtype=np.float32) / np.float32(pairs))).astype(np.float32)
    tables = []
    for count, lane in ((NZ * NY * NC * 8, 0), (GRID, pairs)):
        angle = np.arange(count, dtype=np.float32)[:, None] * inv_freq[None, :]
        cosine = np.zeros((count, HEAD), np.float32)
        sine = np.zeros((count, HEAD), np.float32)
        for start, sign in ((lane, -1.0), (lane + HEAD // 2, 1.0)):
            cosine[:, start : start + pairs] = np.cos(angle.astype(np.float64))
            sine[:, start : start + pairs] = sign * np.sin(angle.astype(np.float64))
        tables += [cosine, sine]
    return tables


DOC_ROWS = 16
HALF_ROWS = HEAD + DOC_ROWS + HEAD
PART_ROWS = ((0, HEAD + DOC_ROWS), (HEAD + DOC_ROWS, HEAD))
SAME_DOC = 32768.0


def span(part):
    return (0, HALF_ROWS) if part is None else PART_ROWS[part]


def gather_events():
    first, second, third, fourth = [], [], [], []
    for half in (0, 1):
        first += [(half, 0, 1, None), (half, 0, -1, None), (half, 1, 0, None), (half, -1, 0, None)]
        second += [(half, 0, 2, 0), (half, 0, 2, 1), (half, 2, 0, 0), (half, 2, 0, 1)]
        third += [(half, i, j, None) for j in (1, -1) for i in (1, -1)]
        fourth += [(half, i, 2, p) for p in (0, 1) for i in (1, -1)]
        fourth += [(half, 2, j, p) for j in (1, -1) for p in (0, 1)]
    last = [(half, 2, 2, p) for p in (0, 1) for half in (0, 1)]
    return first + second + third + fourth + last


EVENTS = gather_events()
EVENT_ID = {e: n for n, e in enumerate(EVENTS)}
UNITS = [(0, (0, 0)), (1, (0, 0)), (0, (0, -1)), (0, (0, 1)), (0, (-1, 0)), (0, (1, 0)), (1, (-1, 0)), (1, (1, 0)), (1, (0, -1)), (1, (0, 1)), (0, (0, 2)), (0, (-1, -1)), (0, (1, -1)), (1, (-1, -1)), (1, (-1, 1)), (0, (-1, 1)), (0, (1, 1)), (0, (2, 0)), (1, (1, -1)), (1, (1, 1)), (1, (2, 0)), (1, (0, 2)), (1, (-1, 2)), (0, (1, 2)), (0, (-1, 2)), (1, (1, 2)), (0, (2, -1)), (1, (2, 1)), (0, (2, 1)), (1, (2, -1)), (0, (2, 2)), (1, (2, 2))]
GAPS = [[], [0, 1, 2, 3], [4, 5, 6, 7], [9, 8], [16, 17], [20, 21, 18, 19], [11, 10, 22, 23], [13, 12, 15, 14], [27, 26, 37, 36, 25, 39, 24], [38, 29, 35, 28, 34], [31, 33, 30, 32, 42], [40, 43], [41], [], [], []]
UNIT_ID = {unit: n for n, unit in enumerate(UNITS)}


def sends_of(event):
    half, i, j, part = event
    out = []
    if i == 0 and j == 0:
        out += [(0, s, (half, 0, s, None)) for s in (1, -1)]
        out += [(1, s, (half, s, 0, None)) for s in (1, -1)]
    elif i == 0:
        if j == 1:
            out.append((0, 1, (half, 0, 2, 0)))
        if j == -1:
            out.append((0, -1, (half, 0, 2, 1)))
        out += [(1, s, (half, s, j, part)) for s in (1, -1)]
    elif i == 1 and part in (None, 0):
        out.append((1, 1, (half, 2, j, 0)))
    elif i == -1 and part in (None, 1):
        out.append((1, -1, (half, 2, j, 1)))
    return out


def unit_of(event):
    half, i, j, part = event
    wrap = lambda v: (v + 1) % 4 - 1
    return UNIT_ID[(half, (wrap(-i), wrap(-j)) if half == 0 else (wrap(-j), wrap(-i)))]


OWN = ((0, 0, 0, None), (1, 0, 0, None))
SENDS = [(e, axis, step, target) for e in list(OWN) + EVENTS for axis, step, target in sends_of(e)]


GROUPS = 4
DEVICES = NZ * NY * NC * NX
PER_GROUP = DEVICES // GROUPS


def exchange_order():
    every = [(a, b, c, d) for a in range(NZ) for b in range(NY) for c in range(NC) for d in range(NX)]
    far = lambda o: min(o[0], NZ - o[0]) + min(o[1], NY - o[1]) + min(o[3], NX - o[3])
    others = [o for o in every if any(o)]
    return sorted(others, key=lambda o: (-far(o), o[3], o[1], o[0], o[2])) + [(0, 0, 0, 0)]


ORDER = exchange_order()


def order_table():
    table = np.zeros((1, DEVICES), np.float32)
    for n, (dz, dy, dc, dx) in enumerate(ORDER):
        table[0, ((dz * NY + dy) * NC + dc) * NX + dx] = n
    return table


def norm_rows(stream, gain, bias):
    center = jnp.mean(stream, axis=-1, keepdims=True)
    spread = jnp.mean(jnp.square(stream - center), axis=-1, keepdims=True)
    return (stream - center) * lax.rsqrt(spread + eps_norm) * gain + bias


def layer_kernel(
    query_hbm, key_hbm, value_hbm, docs_hbm, qgain_hbm, kgain_hbm, rowc_hbm, rows_hbm, colc_hbm, cols_hbm,
    res_hbm, routes_hbm, weights_hbm, order_hbm, ogain_hbm, mgain_hbm, mbias_hbm, fgain_hbm, fbias_hbm,
    proj_hbm, gate_hbm, up_hbm, down_hbm,
    out_ref,
    query_ref, key_ref, docs_ref, qgain_ref, kgain_ref, rowc_ref, rows_ref, colc_ref, cols_ref,
    res_ref, routes_ref, weights_ref, order_ref, ogain_ref, mgain_ref, mbias_ref, fgain_ref, fbias_ref,
    proj, gate, up, down,
    slots, queries, acc, top, low, slot_columns, weight_columns, slot_rows, choose,
    att_ref, att_buf, stream, mid, sent, got, served, back, picked, xs,
    load_sem, send_sem, recv_sem, pair_send, pair_recv, att_send, att_recv, go_send, go_recv, ret_send, ret_recv,
):
    sp, tp = lax.axis_index("sp"), lax.axis_index("tp")
    core = sp % NC
    y = (sp // NC) % NY
    z = sp // (NC * NY)
    rows = key_ref.shape[0]
    half_rows = rows // 2
    heads = query_ref.shape[1] // HEAD
    tokens, width = res_ref.shape
    chunks = width // WIDE
    block = CAP * chunks
    group_rows = PER_GROUP * block
    zs = [((z + d) % NZ) * (NY * NC) for d in range(NZ)]
    ys = [((y + d) % NY) * NC for d in range(NY)]
    cs = [(core + d) % NC for d in range(NC)]
    xs_at = [(tp + d) % NX for d in range(NX)]
    partner = sp + 1 - 2 * core
    near = {}
    for step in (1, -1):
        near[True, step] = z * (NY * NC) + ((y + NY + step) % NY) * NC + core
        near[False, step] = ((z + NZ + step) % NZ) * (NY * NC) + y * NC + core

    barrier = pltpu.get_barrier_semaphore()

    @pl.loop(1, DEVICES)
    def _(n):
        to_sp = ((z + n // (NY * NC * NX)) % NZ) * (NY * NC) + ((y + n // (NC * NX)) % NY) * NC + (core + n // NX) % NC
        pl.semaphore_signal(barrier, inc=1, device_id=(to_sp, (tp + n) % NX), device_id_type=MESH)

    first = (key_hbm, docs_hbm, kgain_hbm, rowc_hbm, rows_hbm, colc_hbm, cols_hbm)
    first_in = (key_ref, docs_ref, kgain_ref, rowc_ref, rows_ref, colc_ref, cols_ref)
    later = (query_hbm, qgain_hbm, routes_hbm, weights_hbm, order_hbm, res_hbm, ogain_hbm, mgain_hbm, mbias_hbm, fgain_hbm, fbias_hbm)
    later_in = (query_ref, qgain_ref, routes_ref, weights_ref, order_ref, res_ref, ogain_ref, mgain_ref, mbias_ref, fgain_ref, fbias_ref)
    last = (proj_hbm, gate_hbm.at[0], up_hbm.at[0], down_hbm.at[0])
    last_in = (proj, gate, up, down)
    pairs = list(zip(first + later + last, first_in + later_in + last_in))
    loads = [pltpu.make_async_copy(src, dst, load_sem.at[n]) for n, (src, dst) in enumerate(pairs)]
    first_loads, later_loads, last_loads = loads[: len(first)], loads[len(first) : len(first + later)], loads[len(first + later) :]
    value_loads = [
        pltpu.make_async_copy(
            value_hbm.at[pl.ds(h * half_rows + k * HEAD, HEAD), :],
            slots.at[unit_of(OWN[h]), 0, pl.ds(HEAD + DOC_ROWS, HEAD), pl.ds(k * HEAD, HEAD)],
            load_sem.at[len(pairs) + 2 * h + k],
        )
        for h in range(2)
        for k in range(2)
    ]
    for load in first_loads + value_loads + later_loads + last_loads:
        load.start()
    for load in first_loads:
        load.wait()

    def table(row_ref, col_ref):
        mine = row_ref[pl.ds(pl.multiple_of(sp * 8, 8), 8), :]
        return jnp.concatenate([col_ref[...] + mine[n : n + 1, :] for n in range(8)], axis=0)

    cosine, sine = table(rowc_ref, colc_ref), table(rows_ref, cols_ref)
    turned = turn(key_ref[...].astype(jnp.float32), kgain_ref[...], cosine, sine).astype(jnp.float32)
    numbers = lax.broadcasted_iota(jnp.int32, (HEAD, half_rows), 0)
    for h in range(2):
        part = slice(h * half_rows, (h + 1) * half_rows)
        unit = unit_of(OWN[h])
        slots[unit, 0, 0:HEAD, :] = jnp.transpose(turned[part, :]).astype(jnp.bfloat16)
        same = (numbers[0:DOC_ROWS, :] == docs_ref[:, h * half_rows : (h + 1) * half_rows]).astype(jnp.float32)
        slots[unit, 0, HEAD : HEAD + DOC_ROWS, :] = same.astype(jnp.bfloat16)
    for load in value_loads:
        load.wait()
    pl.semaphore_wait(barrier, DEVICES - 1)

    def sent_copy(number):
        event, axis, step, target = SENDS[number]
        half = event[0]
        start, size = span(target[3])
        return pltpu.make_async_remote_copy(
            src_ref=slots.at[unit_of(event), 0, pl.ds(start, size), :],
            dst_ref=slots.at[unit_of(target), 0, pl.ds(start, size), :],
            send_sem=send_sem.at[number],
            recv_sem=recv_sem.at[EVENT_ID[target]],
            device_id=(near[(axis == 0) == (half == 0), step], tp),
            device_id_type=MESH,
        )

    def pair_copy(event, number):
        start, size = span(event[3])
        return pltpu.make_async_remote_copy(
            src_ref=slots.at[unit_of(event), 0, pl.ds(start, size), :],
            dst_ref=slots.at[unit_of(event), 1, pl.ds(start, size), :],
            send_sem=pair_send.at[number],
            recv_sem=pair_recv.at[unit_of(event)],
            device_id=(partner, tp),
            device_id_type=MESH,
        )

    def pass_on(event):
        for number, entry in enumerate(SENDS):
            if entry[0] == event:
                sent_copy(number).start()
        pair_copy(event, (list(OWN) + EVENTS).index(event)).start()

    for event in OWN:
        pass_on(event)
    for load in later_loads:
        load.wait()

    columns = [jnp.transpose((numbers == docs_ref[:, h * half_rows : (h + 1) * half_rows]).astype(jnp.float32)) for h in range(2)]
    same = (jnp.concatenate(columns, axis=0) * SAME_DOC).astype(jnp.bfloat16)
    for head in range(heads):
        queries[head, :, 0:HEAD] = turn(
            query_ref[:, head * HEAD : (head + 1) * HEAD].astype(jnp.float32), qgain_ref[...], cosine, sine
        )
        queries[head, :, HEAD:] = same[:, 0:DOC_ROWS]
    lane = lax.broadcasted_iota(jnp.int32, (tokens, DEVICES), 1)

    def column(row):
        return jnp.transpose(jnp.broadcast_to(row, (DEVICES, tokens)))

    named = [column(routes_ref[k : k + 1, :].astype(jnp.float32)).astype(jnp.int32) for k in (0, 1)]
    hot = [(e == lane).astype(jnp.float32) for e in named]
    earlier = (lax.broadcasted_iota(jnp.int32, (tokens, tokens), 1) < lax.broadcasted_iota(jnp.int32, (tokens, tokens), 0)).astype(
        jnp.float32
    )
    counted = jnp.dot(
        earlier.astype(jnp.bfloat16), (hot[0] + hot[1]).astype(jnp.bfloat16), preferred_element_type=jnp.float32
    )
    for k in (0, 1):
        rank = jnp.sum(hot[k] * counted, axis=1, keepdims=True)
        e = named[k]
        dx = ((e & 3) + NX - tp) & 3
        dc = (((e >> 2) & 1) + core) & 1
        dy = (((e >> 3) & 3) + NY - y) & 3
        dz = ((e >> 5) + NZ - z) & 3
        relative = ((dz * NY + dy) * NC + dc) * NX + dx
        place = jnp.sum(jnp.where(relative == lane, order_ref[...], 0.0), axis=1, keepdims=True)
        slot = jnp.broadcast_to(place * block + rank, (tokens, DEVICES))
        slot_columns[k] = slot.astype(jnp.int32)
        weight_columns[k] = column(weights_ref[k : k + 1, :])
        slot_rows[k] = jnp.transpose(slot)[0:8, :].astype(jnp.int32)
    slot_row = [
        jnp.concatenate([slot_rows[k, 0:1, :] + CAP * c for c in range(chunks)], axis=1) for k in (0, 1)
    ]
    for g in range(GROUPS):
        at_row = lax.broadcasted_iota(jnp.int32, (group_rows, chunks * tokens), 0) + g * group_rows
        taken = (at_row == slot_row[0]) | (at_row == slot_row[1])
        choose[g * group_rows : (g + 1) * group_rows, :] = taken.astype(jnp.float32).astype(jnp.bfloat16)
    acc[...] = jnp.zeros_like(acc)
    low[...] = jnp.zeros_like(low)
    top[...] = jnp.full_like(top, -1e20)

    def advance(k):
        places = [(2 * k + n, c) for n in range(2) for c in range(2)]
        keys = jnp.concatenate([slots[u, c, 0 : HEAD + DOC_ROWS, :] for u, c in places], axis=1)
        values = jnp.concatenate(
            [slots[u, c, HEAD + DOC_ROWS :, n * HEAD : (n + 1) * HEAD] for u, c in places for n in range(2)], axis=0
        )
        lanes = keys.shape[1] // HEAD
        scores = [jnp.dot(queries[h], keys, preferred_element_type=jnp.float32) for h in range(heads)]
        for h in range(heads):
            old = top[h]
            new = jnp.maximum(old, jnp.max(scores[h], axis=1, keepdims=True))
            rescale = jnp.exp2((old - new) * LOG2_SCALE)
            weights = jnp.exp2((scores[h] - jnp.concatenate([new] * lanes, axis=1)) * LOG2_SCALE)
            sums = weights[:, 0:HEAD]
            for n in range(1, lanes):
                sums = sums + weights[:, n * HEAD : (n + 1) * HEAD]
            low[h] = low[h] * rescale + sums
            top[h] = new
            acc[h] = acc[h] * rescale + jnp.dot(
                weights.astype(jnp.bfloat16), values, preferred_element_type=jnp.float32
            )

    def step(k, carry):
        for n, gap in enumerate(GAPS):

            @pl.when(k == n)
            def _(n=n, gap=gap):
                for number in gap:
                    event = EVENTS[number]
                    start, size = span(event[3])
                    here = slots.at[unit_of(event), 0, pl.ds(start, size), :]
                    pltpu.make_async_copy(here, here, recv_sem.at[number]).wait()
                    pass_on(event)
                for unit in (2 * n, 2 * n + 1):
                    here = slots.at[unit, 1, :, :]
                    pltpu.make_async_copy(here, here, pair_recv.at[unit]).wait()

        advance(k)
        return carry

    lax.fori_loop(0, len(GAPS), step, 0)
    for h in range(heads):
        total = jnp.sum(low[h], axis=1, keepdims=True)
        att_ref[:, h * HEAD : (h + 1) * HEAD] = (acc[h] / total).astype(jnp.bfloat16)
    copies = []
    for j in range(1, NX):
        to = (tp + j) % NX
        copy = pltpu.make_async_remote_copy(
            src_ref=att_ref.at[pl.ds(pl.multiple_of(to * tokens, tokens), tokens), :],
            dst_ref=att_buf.at[j],
            send_sem=att_send.at[j],
            recv_sem=att_recv.at[j],
            device_id=(sp, to),
            device_id_type=MESH,
        )
        copy.start()
        copies.append(copy)

    last_loads[0].wait()
    squares = jnp.zeros((tokens, 1), jnp.float32)
    local = att_ref.shape[1]
    for j in range(NX):
        source = (tp + NX - j) % NX
        if j == 0:
            part = att_ref[pl.ds(pl.multiple_of(tp * tokens, tokens), tokens), :]
        else:
            copies[j - 1].wait_recv()
            part = att_buf[j]
        part = part.astype(jnp.float32)
        squares = squares + jnp.sum(part * part, axis=1, keepdims=True)
        gain = ogain_ref[:, pl.ds(pl.multiple_of(source * local, local), local)]
        scaled = (part * gain).astype(jnp.bfloat16)
        product = jnp.dot(
            scaled, proj[pl.ds(pl.multiple_of(source * local, local), local), :], preferred_element_type=jnp.float32
        )
        if j == 0:
            stream[...] = product
        else:
            stream[...] += product
    inv_rms = lax.rsqrt(squares / (NX * local) + eps_norm)

    step_rows = 16
    for n in range(tokens // step_rows):
        part = slice(n * step_rows, (n + 1) * step_rows)
        value = alpha_mix * res_ref[part, :].astype(jnp.float32) + stream[part, :] * inv_rms[part, :]
        value = norm_rows(value, mgain_ref[...], mbias_ref[...]).astype(jnp.bfloat16)
        for c in range(chunks):
            mid[c * tokens + n * step_rows : c * tokens + (n + 1) * step_rows, :] = value[:, c * WIDE : (c + 1) * WIDE]

    def exchange(g, source, target, sends, receives, sign):
        for n in range(g * PER_GROUP, (g + 1) * PER_GROUP):
            dz, dy, dc, dx = ORDER[n]
            if not any(ORDER[n]):
                continue
            at = pl.ds(n * block, block)
            pltpu.make_async_remote_copy(
                src_ref=source.at[at, :],
                dst_ref=target.at[at, :],
                send_sem=sends.at[g],
                recv_sem=receives.at[g],
                device_id=(zs[sign * dz % NZ] + ys[sign * dy % NY] + cs[dc], xs_at[sign * dx % NX]),
                device_id_type=MESH,
            ).start()

    for g in range(GROUPS):
        sent[g * group_rows : (g + 1) * group_rows, :] = jnp.dot(
            choose[g * group_rows : (g + 1) * group_rows, :], mid[...], preferred_element_type=jnp.float32
        ).astype(jnp.bfloat16)
        exchange(g, sent, got, go_send, go_recv, 1)

    own_block = slice((DEVICES - 1) * block, DEVICES * block)
    got[own_block, :] = sent[own_block, :]
    for load in last_loads[1:]:
        load.wait()

    def whole(ref, g):
        return ref.at[pl.ds(g * group_rows, group_rows - (block if g == GROUPS - 1 else 0)), :]

    sub = 256
    ii = lax.broadcasted_iota(jnp.int32, (sub, sub), 0)
    jj = lax.broadcasted_iota(jnp.int32, (sub, sub), 1)
    per_chunk = sub // chunks

    def spot(i):
        return ((i % per_chunk) // CAP) * block + (i // per_chunk) * CAP + i % CAP

    collect = (jj == spot(ii)).astype(jnp.float32).astype(jnp.bfloat16)
    scatter = (ii == spot(jj)).astype(jnp.float32).astype(jnp.bfloat16)
    for g in range(GROUPS):
        pltpu.make_async_copy(whole(got, g), whole(got, g), go_recv.at[g]).wait()
        for s in range(group_rows // sub):
            ordered = jnp.dot(
                collect, got[g * group_rows + s * sub : g * group_rows + (s + 1) * sub, :], preferred_element_type=jnp.float32
            ).astype(jnp.bfloat16)
            for c in range(chunks):
                xs[s * per_chunk : (s + 1) * per_chunk, c * WIDE : (c + 1) * WIDE] = ordered[
                    c * per_chunk : (c + 1) * per_chunk, :
                ]
        x = xs[...]
        gate_part = jnp.dot(x, gate[...], preferred_element_type=jnp.float32)
        up_part = jnp.dot(x, up[...], preferred_element_type=jnp.float32)
        hidden = (gate_part / (1.0 + jnp.exp(-gate_part)) * up_part).astype(jnp.bfloat16)
        result = jnp.dot(hidden, down[...], preferred_element_type=jnp.float32).astype(jnp.bfloat16)
        for s in range(group_rows // sub):
            stacked = jnp.concatenate(
                [result[s * per_chunk : (s + 1) * per_chunk, c * WIDE : (c + 1) * WIDE] for c in range(chunks)], axis=0
            )
            served[g * group_rows + s * sub : g * group_rows + (s + 1) * sub, :] = jnp.dot(
                scatter, stacked, preferred_element_type=jnp.float32
            ).astype(jnp.bfloat16)

        exchange(g, served, back, ret_send, ret_recv, -1)

    back[own_block, :] = served[own_block, :]

    for g in range(GROUPS):
        pltpu.make_async_copy(whole(back, g), whole(back, g), ret_recv.at[g]).wait()
        lanes = lax.broadcasted_iota(jnp.int32, (tokens, group_rows), 1) + g * group_rows
        arrived = back[g * group_rows : (g + 1) * group_rows, :]
        for c in range(chunks):
            total = jnp.zeros((tokens, WIDE), jnp.float32)
            for k in (0, 1):
                mine = (lanes == slot_columns[k, :, 0:1] + CAP * c).astype(jnp.float32).astype(jnp.bfloat16)
                total = total + weight_columns[k, :, 0:1] * jnp.dot(mine, arrived, preferred_element_type=jnp.float32)
            if g == 0:
                picked[:, c * WIDE : (c + 1) * WIDE] = total
            else:
                picked[:, c * WIDE : (c + 1) * WIDE] += total

    for n in range(tokens // step_rows):
        part = slice(n * step_rows, (n + 1) * step_rows)
        value = jnp.concatenate(
            [mid[c * tokens + n * step_rows : c * tokens + (n + 1) * step_rows, :] for c in range(chunks)], axis=1
        )
        value = alpha_mix * value.astype(jnp.float32) + picked[part, :]
        out_ref[part, :] = norm_rows(value, fgain_ref[...], fbias_ref[...]).astype(jnp.bfloat16)

    for copy in copies:
        copy.wait_send()
    for g in range(GROUPS):
        pltpu.make_async_copy(whole(sent, g), whole(sent, g), go_send.at[g]).wait()
        pltpu.make_async_copy(whole(served, g), whole(served, g), ret_send.at[g]).wait()
    for number in range(len(SENDS)):
        sent_copy(number).wait_send()
    for number, event in enumerate(list(OWN) + EVENTS):
        pair_copy(event, number).wait_send()


def per_device(
    queries, key_heads, value_heads, documents, query_gain, key_gain, out_gain, out_proj, residual, mid_gain, mid_bias,
    routes, route_weights, expert_gate, expert_up, expert_down, final_gain, final_bias,
):
    rows = queries.shape[0]
    heads = queries.shape[1] // HEAD
    tokens, width = residual.shape
    chunks = width // WIDE
    slots = DEVICES * CAP * chunks
    vec = lambda v: v.reshape(1, -1)
    tables = [jnp.asarray(t) for t in table_constants()]
    inputs = (
        queries, key_heads, value_heads, vec(documents), vec(query_gain), vec(key_gain), *tables,
        residual, routes.T, route_weights.T, jnp.asarray(order_table()), vec(out_gain), vec(mid_gain), vec(mid_bias),
        vec(final_gain), vec(final_bias), out_proj, expert_gate, expert_up, expert_down,
    )
    held = [v for n, v in enumerate(inputs) if n != 2]
    f32, bf16, i32 = jnp.float32, jnp.bfloat16, jnp.int32
    dma = pltpu.SemaphoreType.DMA
    return pl.pallas_call(
        layer_kernel,
        out_shape=jax.ShapeDtypeStruct((tokens, width), bf16),
        in_specs=[ANY] * len(inputs),
        out_specs=VMEM,
        scratch_shapes=[pltpu.VMEM(v.shape[-2:], v.dtype) for v in held]
        + [
            pltpu.VMEM((len(UNITS), NC, HALF_ROWS, 2 * HEAD), bf16),
            pltpu.VMEM((heads, rows, HEAD + DOC_ROWS), bf16),
            pltpu.VMEM((heads, rows, HEAD), f32),
            pltpu.VMEM((heads, rows, HEAD), f32),
            pltpu.VMEM((heads, rows, HEAD), f32),
            pltpu.VMEM((2, tokens, DEVICES), i32),
            pltpu.VMEM((2, tokens, DEVICES), f32),
            pltpu.VMEM((2, 8, tokens), i32),
            pltpu.VMEM((slots, chunks * tokens), bf16),
            pltpu.VMEM((rows, heads * HEAD), bf16),
            pltpu.VMEM((NX, tokens, heads * HEAD), bf16),
            pltpu.VMEM((tokens, width), f32),
            pltpu.VMEM((chunks * tokens, WIDE), bf16),
            pltpu.VMEM((slots, WIDE), bf16),
            pltpu.VMEM((slots, WIDE), bf16),
            pltpu.VMEM((slots, WIDE), bf16),
            pltpu.VMEM((slots, WIDE), bf16),
            pltpu.VMEM((tokens, width), f32),
            pltpu.VMEM((tokens, width), bf16),
            dma((len(inputs) + 3,)),
            dma((len(SENDS),)),
            dma((len(EVENTS),)),
            dma((len(EVENTS) + 2,)),
            dma((len(UNITS),)),
            dma((NX,)),
            dma((NX,)),
            dma((GROUPS,)),
            dma((GROUPS,)),
            dma((GROUPS,)),
            dma((GROUPS,)),
        ],
        compiler_params=pltpu.CompilerParams(
            collective_id=0, has_side_effects=True, vmem_limit_bytes=60 * 1024 * 1024
        ),
        name="layer",
    )(*inputs)


def solution(mesh):
    both = ("sp", "tp")
    return jax.shard_map(
        per_device,
        mesh=mesh,
        in_specs=(
            P("sp", "tp"),
            P("sp", "tp"),
            P("sp", "tp"),
            P("sp"),
            P(),
            P(),
            P(),
            P(),
            P(both, None),
            P(),
            P(),
            P(both, None),
            P(both, None),
            P(both, None, None),
            P(both, None, None),
            P(both, None, None),
            P(),
            P(),
        ),
        out_specs=P(both, None),
        check_vma=False,
    )
```

```python
import functools
import math

import jax
import jax.numpy as jnp
import numpy as np
from jax import lax
from jax.experimental import pallas as pl
from jax.experimental.pallas import tpu as pltpu
from jax.sharding import PartitionSpec as P

HEAD = 128
GRID = 64

eps_norm = 1e-06
alpha_mix = 8.0**0.25
theta_base = 10000.0
LOG2_SCALE = HEAD ** (-0.5) * math.log2(math.e)

ANY = pl.BlockSpec(memory_space=pl.ANY)
VMEM = pl.BlockSpec(memory_space=pltpu.VMEM)


def turn(values, gain, cosine, sine):
    inv_rms = lax.rsqrt(jnp.mean(values * values, axis=-1, keepdims=True) + eps_norm)
    values = values * inv_rms * gain
    swapped = pltpu.roll(values, HEAD // 2, 1)
    return (values * cosine + swapped * sine).astype(jnp.bfloat16)


NZ, NY, NC, NX = 4, 4, 2, 4
CAP = 4
WIDE = 512
MESH = pl.DeviceIdType.MESH


def table_constants():
    pairs = HEAD // 4
    inv_freq = (theta_base ** (-np.arange(pairs, dtype=np.float32) / np.float32(pairs))).astype(np.float32)
    tables = []
    for count, lane in ((NZ * NY * NC * 8, 0), (GRID, pairs)):
        angle = np.arange(count, dtype=np.float32)[:, None] * inv_freq[None, :]
        cosine = np.zeros((count, HEAD), np.float32)
        sine = np.zeros((count, HEAD), np.float32)
        for start, sign in ((lane, -1.0), (lane + HEAD // 2, 1.0)):
            cosine[:, start : start + pairs] = np.cos(angle.astype(np.float64))
            sine[:, start : start + pairs] = sign * np.sin(angle.astype(np.float64))
        tables += [cosine, sine]
    return tables


DOC_ROWS = 16
HALF_ROWS = HEAD + DOC_ROWS + HEAD
PART_ROWS = ((0, HEAD + DOC_ROWS), (HEAD + DOC_ROWS, HEAD))
SAME_DOC = 32768.0


def span(part):
    return (0, HALF_ROWS) if part is None else PART_ROWS[part]


def gather_events():
    first, second, third, fourth = [], [], [], []
    for half in (0, 1):
        first += [(half, 0, 1, None), (half, 0, -1, None), (half, 1, 0, None), (half, -1, 0, None)]
        second += [(half, 0, 2, 0), (half, 0, 2, 1), (half, 2, 0, 0), (half, 2, 0, 1)]
        third += [(half, i, j, None) for j in (1, -1) for i in (1, -1)]
        fourth += [(half, i, 2, p) for p in (0, 1) for i in (1, -1)]
        fourth += [(half, 2, j, p) for j in (1, -1) for p in (0, 1)]
    last = [(half, 2, 2, p) for p in (0, 1) for half in (0, 1)]
    return first + second + third + fourth + last


EVENTS = gather_events()
EVENT_ID = {e: n for n, e in enumerate(EVENTS)}
UNITS = [(0, (0, 0)), (1, (0, 0)), (0, (0, -1)), (0, (0, 1)), (0, (-1, 0)), (0, (1, 0)), (1, (-1, 0)), (1, (1, 0)), (1, (0, -1)), (1, (0, 1)), (0, (0, 2)), (0, (-1, -1)), (0, (1, -1)), (1, (-1, -1)), (1, (-1, 1)), (0, (-1, 1)), (0, (1, 1)), (0, (2, 0)), (1, (1, -1)), (1, (1, 1)), (1, (2, 0)), (1, (0, 2)), (1, (-1, 2)), (0, (1, 2)), (0, (-1, 2)), (1, (1, 2)), (0, (2, -1)), (1, (2, 1)), (0, (2, 1)), (1, (2, -1)), (0, (2, 2)), (1, (2, 2))]
GAPS = [[], [0, 1, 2, 3], [4, 5, 6, 7], [9, 8], [16, 17], [20, 21, 18, 19], [11, 10, 22, 23], [13, 12, 15, 14], [27, 26, 37, 36, 25, 39, 24], [38, 29, 35, 28, 34], [31, 33, 30, 32, 42], [40, 43], [41], [], [], []]
UNIT_ID = {unit: n for n, unit in enumerate(UNITS)}


def sends_of(event):
    half, i, j, part = event
    out = []
    if i == 0 and j == 0:
        out += [(0, s, (half, 0, s, None)) for s in (1, -1)]
        out += [(1, s, (half, s, 0, None)) for s in (1, -1)]
    elif i == 0:
        if j == 1:
            out.append((0, 1, (half, 0, 2, 0)))
        if j == -1:
            out.append((0, -1, (half, 0, 2, 1)))
        out += [(1, s, (half, s, j, part)) for s in (1, -1)]
    elif i == 1 and part in (None, 0):
        out.append((1, 1, (half, 2, j, 0)))
    elif i == -1 and part in (None, 1):
        out.append((1, -1, (half, 2, j, 1)))
    return out


def unit_of(event):
    half, i, j, part = event
    wrap = lambda v: (v + 1) % 4 - 1
    return UNIT_ID[(half, (wrap(-i), wrap(-j)) if half == 0 else (wrap(-j), wrap(-i)))]


OWN = ((0, 0, 0, None), (1, 0, 0, None))
SENDS = [(e, axis, step, target) for e in list(OWN) + EVENTS for axis, step, target in sends_of(e)]


GROUPS = 4
DEVICES = NZ * NY * NC * NX
PER_GROUP = DEVICES // GROUPS


def exchange_order():
    every = [(a, b, c, d) for a in range(NZ) for b in range(NY) for c in range(NC) for d in range(NX)]
    far = lambda o: min(o[0], NZ - o[0]) + min(o[1], NY - o[1]) + min(o[3], NX - o[3])
    others = [o for o in every if any(o)]
    return sorted(others, key=lambda o: ((sum(o) - o[2]) % GROUPS, -far(o), o)) + [(0, 0, 0, 0)]


ORDER = exchange_order()


def order_table():
    table = np.zeros((1, DEVICES), np.float32)
    for n, (dz, dy, dc, dx) in enumerate(ORDER):
        table[0, ((dz * NY + dy) * NC + dc) * NX + dx] = n
    return table


def norm_rows(stream, gain, bias):
    center = jnp.mean(stream, axis=-1, keepdims=True)
    spread = jnp.mean(jnp.square(stream - center), axis=-1, keepdims=True)
    return (stream - center) * lax.rsqrt(spread + eps_norm) * gain + bias


def layer_kernel(
    query_hbm, key_hbm, value_hbm, docs_hbm, qgain_hbm, kgain_hbm, rowc_hbm, rows_hbm, colc_hbm, cols_hbm,
    res_hbm, routes_hbm, weights_hbm, order_hbm, ogain_hbm, mgain_hbm, mbias_hbm, fgain_hbm, fbias_hbm,
    proj_hbm, gate_hbm, up_hbm, down_hbm,
    out_ref,
    query_ref, key_ref, docs_ref, qgain_ref, kgain_ref, rowc_ref, rows_ref, colc_ref, cols_ref,
    res_ref, routes_ref, weights_ref, order_ref, ogain_ref, mgain_ref, mbias_ref, fgain_ref, fbias_ref,
    proj, gate, up, down,
    slots, queries, acc, top, low, slot_columns, weight_columns, slot_rows, choose,
    att_ref, att_buf, stream, mid, sent, got, served, back, picked, xs,
    load_sem, send_sem, recv_sem, pair_send, pair_recv, att_send, att_recv, go_send, go_recv, ret_send, ret_recv,
):
    sp, tp = lax.axis_index("sp"), lax.axis_index("tp")
    core = sp % NC
    y = (sp // NC) % NY
    z = sp // (NC * NY)
    rows = key_ref.shape[0]
    half_rows = rows // 2
    heads = query_ref.shape[1] // HEAD
    tokens, width = res_ref.shape
    chunks = width // WIDE
    block = CAP * chunks
    group_rows = PER_GROUP * block
    zs = [((z + d) % NZ) * (NY * NC) for d in range(NZ)]
    ys = [((y + d) % NY) * NC for d in range(NY)]
    cs = [(core + d) % NC for d in range(NC)]
    xs_at = [(tp + d) % NX for d in range(NX)]
    partner = sp + 1 - 2 * core
    near = {}
    for step in (1, -1):
        near[True, step] = z * (NY * NC) + ((y + NY + step) % NY) * NC + core
        near[False, step] = ((z + NZ + step) % NZ) * (NY * NC) + y * NC + core

    barrier = pltpu.get_barrier_semaphore()

    for to in list(near.values()) + [partner]:
        pl.semaphore_signal(barrier, inc=1, device_id=(to, tp), device_id_type=MESH)
    for to in xs_at[1:]:
        pl.semaphore_signal(barrier, inc=1, device_id=(sp, to), device_id_type=MESH)

    first = (key_hbm, docs_hbm, kgain_hbm, rowc_hbm, rows_hbm, colc_hbm, cols_hbm)
    first_in = (key_ref, docs_ref, kgain_ref, rowc_ref, rows_ref, colc_ref, cols_ref)
    later = (query_hbm, qgain_hbm, routes_hbm, weights_hbm, order_hbm, res_hbm, ogain_hbm, mgain_hbm, mbias_hbm, fgain_hbm, fbias_hbm)
    later_in = (query_ref, qgain_ref, routes_ref, weights_ref, order_ref, res_ref, ogain_ref, mgain_ref, mbias_ref, fgain_ref, fbias_ref)
    last = (proj_hbm, gate_hbm.at[0], up_hbm.at[0], down_hbm.at[0])
    last_in = (proj, gate, up, down)
    pairs = list(zip(first + later + last, first_in + later_in + last_in))
    loads = [pltpu.make_async_copy(src, dst, load_sem.at[n]) for n, (src, dst) in enumerate(pairs)]
    first_loads, later_loads, last_loads = loads[: len(first)], loads[len(first) : len(first + later)], loads[len(first + later) :]
    value_loads = [
        pltpu.make_async_copy(
            value_hbm.at[pl.ds(h * half_rows + k * HEAD, HEAD), :],
            slots.at[unit_of(OWN[h]), 0, pl.ds(HEAD + DOC_ROWS, HEAD), pl.ds(k * HEAD, HEAD)],
            load_sem.at[len(pairs) + 2 * h + k],
        )
        for h in range(2)
        for k in range(2)
    ]
    for load in first_loads + value_loads + later_loads + last_loads:
        load.start()
    for load in first_loads:
        load.wait()

    def table(row_ref, col_ref):
        mine = row_ref[pl.ds(pl.multiple_of(sp * 8, 8), 8), :]
        return jnp.concatenate([col_ref[...] + mine[n : n + 1, :] for n in range(8)], axis=0)

    cosine, sine = table(rowc_ref, colc_ref), table(rows_ref, cols_ref)
    turned = turn(key_ref[...].astype(jnp.float32), kgain_ref[...], cosine, sine).astype(jnp.float32)
    numbers = lax.broadcasted_iota(jnp.int32, (HEAD, half_rows), 0)
    for h in range(2):
        part = slice(h * half_rows, (h + 1) * half_rows)
        unit = unit_of(OWN[h])
        slots[unit, 0, 0:HEAD, :] = jnp.transpose(turned[part, :]).astype(jnp.bfloat16)
        same = (numbers[0:DOC_ROWS, :] == docs_ref[:, h * half_rows : (h + 1) * half_rows]).astype(jnp.float32)
        slots[unit, 0, HEAD : HEAD + DOC_ROWS, :] = same.astype(jnp.bfloat16)
    for load in value_loads:
        load.wait()
    pl.semaphore_wait(barrier, 5 + NX - 1)

    def sent_copy(number):
        event, axis, step, target = SENDS[number]
        half = event[0]
        start, size = span(target[3])
        return pltpu.make_async_remote_copy(
            src_ref=slots.at[unit_of(event), 0, pl.ds(start, size), :],
            dst_ref=slots.at[unit_of(target), 0, pl.ds(start, size), :],
            send_sem=send_sem.at[number],
            recv_sem=recv_sem.at[EVENT_ID[target]],
            device_id=(near[(axis == 0) == (half == 0), step], tp),
            device_id_type=MESH,
        )

    def pair_copy(event, number):
        start, size = span(event[3])
        return pltpu.make_async_remote_copy(
            src_ref=slots.at[unit_of(event), 0, pl.ds(start, size), :],
            dst_ref=slots.at[unit_of(event), 1, pl.ds(start, size), :],
            send_sem=pair_send.at[number],
            recv_sem=pair_recv.at[unit_of(event)],
            device_id=(partner, tp),
            device_id_type=MESH,
        )

    def pass_on(event):
        for number, entry in enumerate(SENDS):
            if entry[0] == event:
                sent_copy(number).start()
        pair_copy(event, (list(OWN) + EVENTS).index(event)).start()

    for event in OWN:
        pass_on(event)
    for load in later_loads:
        load.wait()

    columns = [jnp.transpose((numbers == docs_ref[:, h * half_rows : (h + 1) * half_rows]).astype(jnp.float32)) for h in range(2)]
    same = (jnp.concatenate(columns, axis=0) * SAME_DOC).astype(jnp.bfloat16)
    for head in range(heads):
        queries[head, :, 0:HEAD] = turn(
            query_ref[:, head * HEAD : (head + 1) * HEAD].astype(jnp.float32), qgain_ref[...], cosine, sine
        )
        queries[head, :, HEAD:] = same[:, 0:DOC_ROWS]
    lane = lax.broadcasted_iota(jnp.int32, (tokens, DEVICES), 1)

    def column(row):
        return jnp.transpose(jnp.broadcast_to(row, (DEVICES, tokens)))

    named = [column(routes_ref[k : k + 1, :].astype(jnp.float32)).astype(jnp.int32) for k in (0, 1)]
    hot = [(e == lane).astype(jnp.float32) for e in named]
    earlier = (lax.broadcasted_iota(jnp.int32, (tokens, tokens), 1) < lax.broadcasted_iota(jnp.int32, (tokens, tokens), 0)).astype(
        jnp.float32
    )
    counted = jnp.dot(
        earlier.astype(jnp.bfloat16), (hot[0] + hot[1]).astype(jnp.bfloat16), preferred_element_type=jnp.float32
    )
    for k in (0, 1):
        rank = jnp.sum(hot[k] * counted, axis=1, keepdims=True)
        e = named[k]
        dx = ((e & 3) + NX - tp) & 3
        dc = (((e >> 2) & 1) + core) & 1
        dy = (((e >> 3) & 3) + NY - y) & 3
        dz = ((e >> 5) + NZ - z) & 3
        relative = ((dz * NY + dy) * NC + dc) * NX + dx
        place = jnp.sum(jnp.where(relative == lane, order_ref[...], 0.0), axis=1, keepdims=True)
        slot = jnp.broadcast_to(place * block + rank, (tokens, DEVICES))
        slot_columns[k] = slot.astype(jnp.int32)
        weight_columns[k] = column(weights_ref[k : k + 1, :])
        slot_rows[k] = jnp.transpose(slot)[0:8, :].astype(jnp.int32)
    slot_row = [
        jnp.concatenate([slot_rows[k, 0:1, :] + CAP * c for c in range(chunks)], axis=1) for k in (0, 1)
    ]
    for g in range(GROUPS):
        at_row = lax.broadcasted_iota(jnp.int32, (group_rows, chunks * tokens), 0) + g * group_rows
        taken = (at_row == slot_row[0]) | (at_row == slot_row[1])
        choose[g * group_rows : (g + 1) * group_rows, :] = taken.astype(jnp.float32).astype(jnp.bfloat16)
    acc[...] = jnp.zeros_like(acc)
    low[...] = jnp.zeros_like(low)
    top[...] = jnp.full_like(top, -1e20)

    def advance(k):
        places = [(2 * k + n, c) for n in range(2) for c in range(2)]
        keys = jnp.concatenate([slots[u, c, 0 : HEAD + DOC_ROWS, :] for u, c in places], axis=1)
        values = jnp.concatenate(
            [slots[u, c, HEAD + DOC_ROWS :, n * HEAD : (n + 1) * HEAD] for u, c in places for n in range(2)], axis=0
        )
        lanes = keys.shape[1] // HEAD
        scores = [jnp.dot(queries[h], keys, preferred_element_type=jnp.float32) for h in range(heads)]
        for h in range(heads):
            old = top[h]
            new = jnp.maximum(old, jnp.max(scores[h], axis=1, keepdims=True))
            rescale = jnp.exp2((old - new) * LOG2_SCALE)
            weights = jnp.exp2((scores[h] - jnp.concatenate([new] * lanes, axis=1)) * LOG2_SCALE)
            sums = weights[:, 0:HEAD]
            for n in range(1, lanes):
                sums = sums + weights[:, n * HEAD : (n + 1) * HEAD]
            low[h] = low[h] * rescale + sums
            top[h] = new
            acc[h] = acc[h] * rescale + jnp.dot(
                weights.astype(jnp.bfloat16), values, preferred_element_type=jnp.float32
            )

    def step(k, carry):
        for n, gap in enumerate(GAPS):

            @pl.when(k == n)
            def _(n=n, gap=gap):
                for number in gap:
                    event = EVENTS[number]
                    start, size = span(event[3])
                    here = slots.at[unit_of(event), 0, pl.ds(start, size), :]
                    pltpu.make_async_copy(here, here, recv_sem.at[number]).wait()
                    pass_on(event)
                for unit in (2 * n, 2 * n + 1):
                    here = slots.at[unit, 1, :, :]
                    pltpu.make_async_copy(here, here, pair_recv.at[unit]).wait()

        advance(k)
        return carry

    lax.fori_loop(0, len(GAPS), step, 0)
    for h in range(heads):
        total = jnp.sum(low[h], axis=1, keepdims=True)
        att_ref[:, h * HEAD : (h + 1) * HEAD] = (acc[h] / total).astype(jnp.bfloat16)
    copies = []
    for j in range(1, NX):
        to = (tp + j) % NX
        copy = pltpu.make_async_remote_copy(
            src_ref=att_ref.at[pl.ds(pl.multiple_of(to * tokens, tokens), tokens), :],
            dst_ref=att_buf.at[j],
            send_sem=att_send.at[j],
            recv_sem=att_recv.at[j],
            device_id=(sp, to),
            device_id_type=MESH,
        )
        copy.start()
        copies.append(copy)

    last_loads[0].wait()
    squares = jnp.zeros((tokens, 1), jnp.float32)
    local = att_ref.shape[1]
    for j in range(NX):
        source = (tp + NX - j) % NX
        if j == 0:
            part = att_ref[pl.ds(pl.multiple_of(tp * tokens, tokens), tokens), :]
        else:
            copies[j - 1].wait_recv()
            part = att_buf[j]
        part = part.astype(jnp.float32)
        squares = squares + jnp.sum(part * part, axis=1, keepdims=True)
        gain = ogain_ref[:, pl.ds(pl.multiple_of(source * local, local), local)]
        scaled = (part * gain).astype(jnp.bfloat16)
        product = jnp.dot(
            scaled, proj[pl.ds(pl.multiple_of(source * local, local), local), :], preferred_element_type=jnp.float32
        )
        if j == 0:
            stream[...] = product
        else:
            stream[...] += product
    inv_rms = lax.rsqrt(squares / (NX * local) + eps_norm)

    step_rows = 16
    for n in range(tokens // step_rows):
        part = slice(n * step_rows, (n + 1) * step_rows)
        value = alpha_mix * res_ref[part, :].astype(jnp.float32) + stream[part, :] * inv_rms[part, :]
        value = norm_rows(value, mgain_ref[...], mbias_ref[...]).astype(jnp.bfloat16)
        for c in range(chunks):
            mid[c * tokens + n * step_rows : c * tokens + (n + 1) * step_rows, :] = value[:, c * WIDE : (c + 1) * WIDE]

    def exchange(g, source, target, sends, receives, sign):
        for n in range(g * PER_GROUP, (g + 1) * PER_GROUP):
            dz, dy, dc, dx = ORDER[n]
            if not any(ORDER[n]):
                continue
            at = pl.ds(n * block, block)
            pltpu.make_async_remote_copy(
                src_ref=source.at[at, :],
                dst_ref=target.at[at, :],
                send_sem=sends.at[g],
                recv_sem=receives.at[g],
                device_id=(zs[sign * dz % NZ] + ys[sign * dy % NY] + cs[dc], xs_at[sign * dx % NX]),
                device_id_type=MESH,
            ).start()

    for g in range(GROUPS):
        sent[g * group_rows : (g + 1) * group_rows, :] = jnp.dot(
            choose[g * group_rows : (g + 1) * group_rows, :], mid[...], preferred_element_type=jnp.float32
        ).astype(jnp.bfloat16)
        exchange(g, sent, got, go_send, go_recv, 1)

    own_block = slice((DEVICES - 1) * block, DEVICES * block)
    got[own_block, :] = sent[own_block, :]
    for load in last_loads[1:]:
        load.wait()

    def whole(ref, g):
        return ref.at[pl.ds(g * group_rows, group_rows - (block if g == GROUPS - 1 else 0)), :]

    sub = 256
    ii = lax.broadcasted_iota(jnp.int32, (sub, sub), 0)
    jj = lax.broadcasted_iota(jnp.int32, (sub, sub), 1)
    per_chunk = sub // chunks

    def spot(i):
        return ((i % per_chunk) // CAP) * block + (i // per_chunk) * CAP + i % CAP

    collect = (jj == spot(ii)).astype(jnp.float32).astype(jnp.bfloat16)
    scatter = (ii == spot(jj)).astype(jnp.float32).astype(jnp.bfloat16)
    for g in range(GROUPS):
        pltpu.make_async_copy(whole(got, g), whole(got, g), go_recv.at[g]).wait()
        for s in range(group_rows // sub):
            ordered = jnp.dot(
                collect, got[g * group_rows + s * sub : g * group_rows + (s + 1) * sub, :], preferred_element_type=jnp.float32
            ).astype(jnp.bfloat16)
            for c in range(chunks):
                xs[s * per_chunk : (s + 1) * per_chunk, c * WIDE : (c + 1) * WIDE] = ordered[
                    c * per_chunk : (c + 1) * per_chunk, :
                ]
        x = xs[...]
        gate_part = jnp.dot(x, gate[...], preferred_element_type=jnp.float32)
        up_part = jnp.dot(x, up[...], preferred_element_type=jnp.float32)
        hidden = (gate_part / (1.0 + jnp.exp(-gate_part)) * up_part).astype(jnp.bfloat16)
        result = jnp.dot(hidden, down[...], preferred_element_type=jnp.float32).astype(jnp.bfloat16)
        for s in range(group_rows // sub):
            stacked = jnp.concatenate(
                [result[s * per_chunk : (s + 1) * per_chunk, c * WIDE : (c + 1) * WIDE] for c in range(chunks)], axis=0
            )
            served[g * group_rows + s * sub : g * group_rows + (s + 1) * sub, :] = jnp.dot(
                scatter, stacked, preferred_element_type=jnp.float32
            ).astype(jnp.bfloat16)

        exchange(g, served, back, ret_send, ret_recv, -1)

    back[own_block, :] = served[own_block, :]

    for g in range(GROUPS):
        pltpu.make_async_copy(whole(back, g), whole(back, g), ret_recv.at[g]).wait()
        lanes = lax.broadcasted_iota(jnp.int32, (tokens, group_rows), 1) + g * group_rows
        arrived = back[g * group_rows : (g + 1) * group_rows, :]
        for c in range(chunks):
            total = jnp.zeros((tokens, WIDE), jnp.float32)
            for k in (0, 1):
                mine = (lanes == slot_columns[k, :, 0:1] + CAP * c).astype(jnp.float32).astype(jnp.bfloat16)
                total = total + weight_columns[k, :, 0:1] * jnp.dot(mine, arrived, preferred_element_type=jnp.float32)
            if g == 0:
                picked[:, c * WIDE : (c + 1) * WIDE] = total
            else:
                picked[:, c * WIDE : (c + 1) * WIDE] += total

    for n in range(tokens // step_rows):
        part = slice(n * step_rows, (n + 1) * step_rows)
        value = jnp.concatenate(
            [mid[c * tokens + n * step_rows : c * tokens + (n + 1) * step_rows, :] for c in range(chunks)], axis=1
        )
        value = alpha_mix * value.astype(jnp.float32) + picked[part, :]
        out_ref[part, :] = norm_rows(value, fgain_ref[...], fbias_ref[...]).astype(jnp.bfloat16)

    for copy in copies:
        copy.wait_send()
    for g in range(GROUPS):
        pltpu.make_async_copy(whole(sent, g), whole(sent, g), go_send.at[g]).wait()
        pltpu.make_async_copy(whole(served, g), whole(served, g), ret_send.at[g]).wait()
    for number in range(len(SENDS)):
        sent_copy(number).wait_send()
    for number, event in enumerate(list(OWN) + EVENTS):
        pair_copy(event, number).wait_send()


def per_device(
    queries, key_heads, value_heads, documents, query_gain, key_gain, out_gain, out_proj, residual, mid_gain, mid_bias,
    routes, route_weights, expert_gate, expert_up, expert_down, final_gain, final_bias,
):
    rows = queries.shape[0]
    heads = queries.shape[1] // HEAD
    tokens, width = residual.shape
    chunks = width // WIDE
    slots = DEVICES * CAP * chunks
    vec = lambda v: v.reshape(1, -1)
    tables = [jnp.asarray(t) for t in table_constants()]
    inputs = (
        queries, key_heads, value_heads, vec(documents), vec(query_gain), vec(key_gain), *tables,
        residual, routes.T, route_weights.T, jnp.asarray(order_table()), vec(out_gain), vec(mid_gain), vec(mid_bias),
        vec(final_gain), vec(final_bias), out_proj, expert_gate, expert_up, expert_down,
    )
    held = [v for n, v in enumerate(inputs) if n != 2]
    f32, bf16, i32 = jnp.float32, jnp.bfloat16, jnp.int32
    dma = pltpu.SemaphoreType.DMA
    return pl.pallas_call(
        layer_kernel,
        out_shape=jax.ShapeDtypeStruct((tokens, width), bf16),
        in_specs=[ANY] * len(inputs),
        out_specs=VMEM,
        scratch_shapes=[pltpu.VMEM(v.shape[-2:], v.dtype) for v in held]
        + [
            pltpu.VMEM((len(UNITS), NC, HALF_ROWS, 2 * HEAD), bf16),
            pltpu.VMEM((heads, rows, HEAD + DOC_ROWS), bf16),
            pltpu.VMEM((heads, rows, HEAD), f32),
            pltpu.VMEM((heads, rows, HEAD), f32),
            pltpu.VMEM((heads, rows, HEAD), f32),
            pltpu.VMEM((2, tokens, DEVICES), i32),
            pltpu.VMEM((2, tokens, DEVICES), f32),
            pltpu.VMEM((2, 8, tokens), i32),
            pltpu.VMEM((slots, chunks * tokens), bf16),
            pltpu.VMEM((rows, heads * HEAD), bf16),
            pltpu.VMEM((NX, tokens, heads * HEAD), bf16),
            pltpu.VMEM((tokens, width), f32),
            pltpu.VMEM((chunks * tokens, WIDE), bf16),
            pltpu.VMEM((slots, WIDE), bf16),
            pltpu.VMEM((slots, WIDE), bf16),
            pltpu.VMEM((slots, WIDE), bf16),
            pltpu.VMEM((slots, WIDE), bf16),
            pltpu.VMEM((tokens, width), f32),
            pltpu.VMEM((tokens, width), bf16),
            dma((len(inputs) + 3,)),
            dma((len(SENDS),)),
            dma((len(EVENTS),)),
            dma((len(EVENTS) + 2,)),
            dma((len(UNITS),)),
            dma((NX,)),
            dma((NX,)),
            dma((GROUPS,)),
            dma((GROUPS,)),
            dma((GROUPS,)),
            dma((GROUPS,)),
        ],
        compiler_params=pltpu.CompilerParams(
            collective_id=0, has_side_effects=True, vmem_limit_bytes=60 * 1024 * 1024
        ),
        name="layer",
    )(*inputs)


def solution(mesh):
    both = ("sp", "tp")
    return jax.shard_map(
        per_device,
        mesh=mesh,
        in_specs=(
            P("sp", "tp"),
            P("sp", "tp"),
            P("sp", "tp"),
            P("sp"),
            P(),
            P(),
            P(),
            P(),
            P(both, None),
            P(),
            P(),
            P(both, None),
            P(both, None),
            P(both, None, None),
            P(both, None, None),
            P(both, None, None),
            P(),
            P(),
        ),
        out_specs=P(both, None),
        check_vma=False,
    )
```

```python
import functools
import math

import jax
import jax.numpy as jnp
import numpy as np
from jax import lax
from jax.experimental import pallas as pl
from jax.experimental.pallas import tpu as pltpu
from jax.sharding import PartitionSpec as P

HEAD = 128
GRID = 64

eps_norm = 1e-06
alpha_mix = 8.0**0.25
theta_base = 10000.0
LOG2_SCALE = HEAD ** (-0.5) * math.log2(math.e)

ANY = pl.BlockSpec(memory_space=pl.ANY)
VMEM = pl.BlockSpec(memory_space=pltpu.VMEM)


def turn(values, gain, cosine, sine):
    inv_rms = lax.rsqrt(jnp.mean(values * values, axis=-1, keepdims=True) + eps_norm)
    values = values * inv_rms * gain
    swapped = pltpu.roll(values, HEAD // 2, 1)
    return (values * cosine + swapped * sine).astype(jnp.bfloat16)


NZ, NY, NC, NX = 4, 4, 2, 4
CAP = 4
WIDE = 512
MESH = pl.DeviceIdType.MESH


def table_constants():
    pairs = HEAD // 4
    inv_freq = (theta_base ** (-np.arange(pairs, dtype=np.float32) / np.float32(pairs))).astype(np.float32)
    tables = []
    for count, lane in ((NZ * NY * NC * 8, 0), (GRID, pairs)):
        angle = np.arange(count, dtype=np.float32)[:, None] * inv_freq[None, :]
        cosine = np.zeros((count, HEAD), np.float32)
        sine = np.zeros((count, HEAD), np.float32)
        for start, sign in ((lane, -1.0), (lane + HEAD // 2, 1.0)):
            cosine[:, start : start + pairs] = np.cos(angle.astype(np.float64))
            sine[:, start : start + pairs] = sign * np.sin(angle.astype(np.float64))
        tables += [cosine, sine]
    return tables


DOC_ROWS = 16
HALF_ROWS = HEAD + DOC_ROWS + HEAD
PART_ROWS = ((0, HEAD + DOC_ROWS), (HEAD + DOC_ROWS, HEAD))
SAME_DOC = 32768.0


def span(part):
    return (0, HALF_ROWS) if part is None else PART_ROWS[part]


def gather_events():
    first, second, third, fourth = [], [], [], []
    for half in (0, 1):
        first += [(half, 0, 1, None), (half, 0, -1, None), (half, 1, 0, None), (half, -1, 0, None)]
        second += [(half, 0, 2, 0), (half, 0, 2, 1), (half, 2, 0, 0), (half, 2, 0, 1)]
        third += [(half, i, j, None) for j in (1, -1) for i in (1, -1)]
        fourth += [(half, i, 2, p) for p in (0, 1) for i in (1, -1)]
        fourth += [(half, 2, j, p) for j in (1, -1) for p in (0, 1)]
    last = [(half, 2, 2, p) for p in (0, 1) for half in (0, 1)]
    return first + second + third + fourth + last


EVENTS = gather_events()
EVENT_ID = {e: n for n, e in enumerate(EVENTS)}
UNITS = [(0, (0, 0)), (1, (0, 0)), (0, (0, -1)), (0, (0, 1)), (0, (-1, 0)), (0, (1, 0)), (1, (-1, 0)), (1, (1, 0)), (1, (0, -1)), (1, (0, 1)), (0, (0, 2)), (0, (-1, -1)), (0, (1, -1)), (1, (-1, -1)), (1, (-1, 1)), (0, (-1, 1)), (0, (1, 1)), (0, (2, 0)), (1, (1, -1)), (1, (1, 1)), (1, (2, 0)), (1, (0, 2)), (1, (-1, 2)), (0, (1, 2)), (0, (-1, 2)), (1, (1, 2)), (0, (2, -1)), (1, (2, 1)), (0, (2, 1)), (1, (2, -1)), (0, (2, 2)), (1, (2, 2))]
GAPS = [[], [0, 1, 2, 3], [4, 5, 6, 7], [9, 8], [16, 17], [20, 21, 18, 19], [11, 10, 22, 23], [13, 12, 15, 14], [27, 26, 37, 36, 25, 39, 24], [38, 29, 35, 28, 34], [31, 33, 30, 32, 42], [40, 43], [41], [], [], []]
UNIT_ID = {unit: n for n, unit in enumerate(UNITS)}


def sends_of(event):
    half, i, j, part = event
    out = []
    if i == 0 and j == 0:
        out += [(0, s, (half, 0, s, None)) for s in (1, -1)]
        out += [(1, s, (half, s, 0, None)) for s in (1, -1)]
    elif i == 0:
        if j == 1:
            out.append((0, 1, (half, 0, 2, 0)))
        if j == -1:
            out.append((0, -1, (half, 0, 2, 1)))
        out += [(1, s, (half, s, j, part)) for s in (1, -1)]
    elif i == 1 and part in (None, 0):
        out.append((1, 1, (half, 2, j, 0)))
    elif i == -1 and part in (None, 1):
        out.append((1, -1, (half, 2, j, 1)))
    return out


def unit_of(event):
    half, i, j, part = event
    wrap = lambda v: (v + 1) % 4 - 1
    return UNIT_ID[(half, (wrap(-i), wrap(-j)) if half == 0 else (wrap(-j), wrap(-i)))]


OWN = ((0, 0, 0, None), (1, 0, 0, None))
SENDS = [(e, axis, step, target) for e in list(OWN) + EVENTS for axis, step, target in sends_of(e)]


GROUPS = 8
DEVICES = NZ * NY * NC * NX
PER_GROUP = DEVICES // GROUPS


def exchange_order():
    every = [(a, b, c, d) for a in range(NZ) for b in range(NY) for c in range(NC) for d in range(NX)]
    far = lambda o: min(o[0], NZ - o[0]) + min(o[1], NY - o[1]) + min(o[3], NX - o[3])
    others = [o for o in every if any(o)]
    return sorted(others, key=lambda o: ((sum(o) - o[2]) % 4, o[2], -far(o), o)) + [(0, 0, 0, 0)]


ORDER = exchange_order()


def order_table():
    table = np.zeros((1, DEVICES), np.float32)
    for n, (dz, dy, dc, dx) in enumerate(ORDER):
        table[0, ((dz * NY + dy) * NC + dc) * NX + dx] = n
    return table


def norm_rows(stream, gain, bias):
    center = jnp.mean(stream, axis=-1, keepdims=True)
    spread = jnp.mean(jnp.square(stream - center), axis=-1, keepdims=True)
    return (stream - center) * lax.rsqrt(spread + eps_norm) * gain + bias


def layer_kernel(
    query_hbm, key_hbm, value_hbm, docs_hbm, qgain_hbm, kgain_hbm, rowc_hbm, rows_hbm, colc_hbm, cols_hbm,
    res_hbm, routes_hbm, weights_hbm, order_hbm, ogain_hbm, mgain_hbm, mbias_hbm, fgain_hbm, fbias_hbm,
    proj_hbm, gate_hbm, up_hbm, down_hbm,
    out_ref,
    query_ref, key_ref, docs_ref, qgain_ref, kgain_ref, rowc_ref, rows_ref, colc_ref, cols_ref,
    res_ref, routes_ref, weights_ref, order_ref, ogain_ref, mgain_ref, mbias_ref, fgain_ref, fbias_ref,
    proj, gate, up, down,
    slots, queries, acc, top, low, slot_columns, weight_columns, slot_rows, choose,
    att_ref, att_buf, stream, mid, sent, got, served, back, picked, xs,
    load_sem, send_sem, recv_sem, pair_send, pair_recv, att_send, att_recv, go_send, go_recv, ret_send, ret_recv,
):
    sp, tp = lax.axis_index("sp"), lax.axis_index("tp")
    core = sp % NC
    y = (sp // NC) % NY
    z = sp // (NC * NY)
    rows = key_ref.shape[0]
    half_rows = rows // 2
    heads = query_ref.shape[1] // HEAD
    tokens, width = res_ref.shape
    chunks = width // WIDE
    block = CAP * chunks
    group_rows = PER_GROUP * block
    zs = [((z + d) % NZ) * (NY * NC) for d in range(NZ)]
    ys = [((y + d) % NY) * NC for d in range(NY)]
    cs = [(core + d) % NC for d in range(NC)]
    xs_at = [(tp + d) % NX for d in range(NX)]
    partner = sp + 1 - 2 * core
    near = {}
    for step in (1, -1):
        near[True, step] = z * (NY * NC) + ((y + NY + step) % NY) * NC + core
        near[False, step] = ((z + NZ + step) % NZ) * (NY * NC) + y * NC + core

    barrier = pltpu.get_barrier_semaphore()

    for to in list(near.values()) + [partner]:
        pl.semaphore_signal(barrier, inc=1, device_id=(to, tp), device_id_type=MESH)
    for to in xs_at[1:]:
        pl.semaphore_signal(barrier, inc=1, device_id=(sp, to), device_id_type=MESH)

    first = (key_hbm, docs_hbm, kgain_hbm, rowc_hbm, rows_hbm, colc_hbm, cols_hbm)
    first_in = (key_ref, docs_ref, kgain_ref, rowc_ref, rows_ref, colc_ref, cols_ref)
    later = (query_hbm, qgain_hbm, routes_hbm, weights_hbm, order_hbm, res_hbm, ogain_hbm, mgain_hbm, mbias_hbm, fgain_hbm, fbias_hbm)
    later_in = (query_ref, qgain_ref, routes_ref, weights_ref, order_ref, res_ref, ogain_ref, mgain_ref, mbias_ref, fgain_ref, fbias_ref)
    last = (proj_hbm, gate_hbm.at[0], up_hbm.at[0], down_hbm.at[0])
    last_in = (proj, gate, up, down)
    pairs = list(zip(first + later + last, first_in + later_in + last_in))
    loads = [pltpu.make_async_copy(src, dst, load_sem.at[n]) for n, (src, dst) in enumerate(pairs)]
    first_loads, later_loads, last_loads = loads[: len(first)], loads[len(first) : len(first + later)], loads[len(first + later) :]
    value_loads = [
        pltpu.make_async_copy(
            value_hbm.at[pl.ds(h * half_rows + k * HEAD, HEAD), :],
            slots.at[unit_of(OWN[h]), 0, pl.ds(HEAD + DOC_ROWS, HEAD), pl.ds(k * HEAD, HEAD)],
            load_sem.at[len(pairs) + 2 * h + k],
        )
        for h in range(2)
        for k in range(2)
    ]
    for load in first_loads + value_loads + later_loads + last_loads:
        load.start()
    for load in first_loads:
        load.wait()

    def table(row_ref, col_ref):
        mine = row_ref[pl.ds(pl.multiple_of(sp * 8, 8), 8), :]
        return jnp.concatenate([col_ref[...] + mine[n : n + 1, :] for n in range(8)], axis=0)

    cosine, sine = table(rowc_ref, colc_ref), table(rows_ref, cols_ref)
    turned = turn(key_ref[...].astype(jnp.float32), kgain_ref[...], cosine, sine).astype(jnp.float32)
    numbers = lax.broadcasted_iota(jnp.int32, (HEAD, half_rows), 0)
    for h in range(2):
        part = slice(h * half_rows, (h + 1) * half_rows)
        unit = unit_of(OWN[h])
        slots[unit, 0, 0:HEAD, :] = jnp.transpose(turned[part, :]).astype(jnp.bfloat16)
        same = (numbers[0:DOC_ROWS, :] == docs_ref[:, h * half_rows : (h + 1) * half_rows]).astype(jnp.float32)
        slots[unit, 0, HEAD : HEAD + DOC_ROWS, :] = same.astype(jnp.bfloat16)
    for load in value_loads:
        load.wait()
    pl.semaphore_wait(barrier, 5 + NX - 1)

    def sent_copy(number):
        event, axis, step, target = SENDS[number]
        half = event[0]
        start, size = span(target[3])
        return pltpu.make_async_remote_copy(
            src_ref=slots.at[unit_of(event), 0, pl.ds(start, size), :],
            dst_ref=slots.at[unit_of(target), 0, pl.ds(start, size), :],
            send_sem=send_sem.at[number],
            recv_sem=recv_sem.at[EVENT_ID[target]],
            device_id=(near[(axis == 0) == (half == 0), step], tp),
            device_id_type=MESH,
        )

    def pair_copy(event, number):
        start, size = span(event[3])
        return pltpu.make_async_remote_copy(
            src_ref=slots.at[unit_of(event), 0, pl.ds(start, size), :],
            dst_ref=slots.at[unit_of(event), 1, pl.ds(start, size), :],
            send_sem=pair_send.at[number],
            recv_sem=pair_recv.at[unit_of(event)],
            device_id=(partner, tp),
            device_id_type=MESH,
        )

    def pass_on(event):
        for number, entry in enumerate(SENDS):
            if entry[0] == event:
                sent_copy(number).start()
        pair_copy(event, (list(OWN) + EVENTS).index(event)).start()

    for event in OWN:
        pass_on(event)
    for load in later_loads:
        load.wait()

    columns = [jnp.transpose((numbers == docs_ref[:, h * half_rows : (h + 1) * half_rows]).astype(jnp.float32)) for h in range(2)]
    same = (jnp.concatenate(columns, axis=0) * SAME_DOC).astype(jnp.bfloat16)
    for head in range(heads):
        queries[head, :, 0:HEAD] = turn(
            query_ref[:, head * HEAD : (head + 1) * HEAD].astype(jnp.float32), qgain_ref[...], cosine, sine
        )
        queries[head, :, HEAD:] = same[:, 0:DOC_ROWS]
    lane = lax.broadcasted_iota(jnp.int32, (tokens, DEVICES), 1)

    def column(row):
        return jnp.transpose(jnp.broadcast_to(row, (DEVICES, tokens)))

    named = [column(routes_ref[k : k + 1, :].astype(jnp.float32)).astype(jnp.int32) for k in (0, 1)]
    hot = [(e == lane).astype(jnp.float32) for e in named]
    earlier = (lax.broadcasted_iota(jnp.int32, (tokens, tokens), 1) < lax.broadcasted_iota(jnp.int32, (tokens, tokens), 0)).astype(
        jnp.float32
    )
    counted = jnp.dot(
        earlier.astype(jnp.bfloat16), (hot[0] + hot[1]).astype(jnp.bfloat16), preferred_element_type=jnp.float32
    )
    for k in (0, 1):
        rank = jnp.sum(hot[k] * counted, axis=1, keepdims=True)
        e = named[k]
        dx = ((e & 3) + NX - tp) & 3
        dc = (((e >> 2) & 1) + core) & 1
        dy = (((e >> 3) & 3) + NY - y) & 3
        dz = ((e >> 5) + NZ - z) & 3
        relative = ((dz * NY + dy) * NC + dc) * NX + dx
        place = jnp.sum(jnp.where(relative == lane, order_ref[...], 0.0), axis=1, keepdims=True)
        slot = jnp.broadcast_to(place * block + rank, (tokens, DEVICES))
        slot_columns[k] = slot.astype(jnp.int32)
        weight_columns[k] = column(weights_ref[k : k + 1, :])
        slot_rows[k] = jnp.transpose(slot)[0:8, :].astype(jnp.int32)
    slot_row = [
        jnp.concatenate([slot_rows[k, 0:1, :] + CAP * c for c in range(chunks)], axis=1) for k in (0, 1)
    ]
    for g in range(GROUPS):
        at_row = lax.broadcasted_iota(jnp.int32, (group_rows, chunks * tokens), 0) + g * group_rows
        taken = (at_row == slot_row[0]) | (at_row == slot_row[1])
        choose[g * group_rows : (g + 1) * group_rows, :] = taken.astype(jnp.float32).astype(jnp.bfloat16)
    acc[...] = jnp.zeros_like(acc)
    low[...] = jnp.zeros_like(low)
    top[...] = jnp.full_like(top, -1e20)

    def advance(k):
        places = [(2 * k + n, c) for n in range(2) for c in range(2)]
        keys = jnp.concatenate([slots[u, c, 0 : HEAD + DOC_ROWS, :] for u, c in places], axis=1)
        values = jnp.concatenate(
            [slots[u, c, HEAD + DOC_ROWS :, n * HEAD : (n + 1) * HEAD] for u, c in places for n in range(2)], axis=0
        )
        lanes = keys.shape[1] // HEAD
        scores = [jnp.dot(queries[h], keys, preferred_element_type=jnp.float32) for h in range(heads)]
        for h in range(heads):
            old = top[h]
            new = jnp.maximum(old, jnp.max(scores[h], axis=1, keepdims=True))
            rescale = jnp.exp2((old - new) * LOG2_SCALE)
            weights = jnp.exp2((scores[h] - jnp.concatenate([new] * lanes, axis=1)) * LOG2_SCALE)
            sums = weights[:, 0:HEAD]
            for n in range(1, lanes):
                sums = sums + weights[:, n * HEAD : (n + 1) * HEAD]
            low[h] = low[h] * rescale + sums
            top[h] = new
            acc[h] = acc[h] * rescale + jnp.dot(
                weights.astype(jnp.bfloat16), values, preferred_element_type=jnp.float32
            )

    def step(k, carry):
        for n, gap in enumerate(GAPS):

            @pl.when(k == n)
            def _(n=n, gap=gap):
                for number in gap:
                    event = EVENTS[number]
                    start, size = span(event[3])
                    here = slots.at[unit_of(event), 0, pl.ds(start, size), :]
                    pltpu.make_async_copy(here, here, recv_sem.at[number]).wait()
                    pass_on(event)
                for unit in (2 * n, 2 * n + 1):
                    here = slots.at[unit, 1, :, :]
                    pltpu.make_async_copy(here, here, pair_recv.at[unit]).wait()

        advance(k)
        return carry

    lax.fori_loop(0, len(GAPS), step, 0)
    for h in range(heads):
        total = jnp.sum(low[h], axis=1, keepdims=True)
        att_ref[:, h * HEAD : (h + 1) * HEAD] = (acc[h] / total).astype(jnp.bfloat16)
    copies = []
    for j in range(1, NX):
        to = (tp + j) % NX
        copy = pltpu.make_async_remote_copy(
            src_ref=att_ref.at[pl.ds(pl.multiple_of(to * tokens, tokens), tokens), :],
            dst_ref=att_buf.at[j],
            send_sem=att_send.at[j],
            recv_sem=att_recv.at[j],
            device_id=(sp, to),
            device_id_type=MESH,
        )
        copy.start()
        copies.append(copy)

    last_loads[0].wait()
    squares = jnp.zeros((tokens, 1), jnp.float32)
    local = att_ref.shape[1]
    for j in range(NX):
        source = (tp + NX - j) % NX
        if j == 0:
            part = att_ref[pl.ds(pl.multiple_of(tp * tokens, tokens), tokens), :]
        else:
            copies[j - 1].wait_recv()
            part = att_buf[j]
        part = part.astype(jnp.float32)
        squares = squares + jnp.sum(part * part, axis=1, keepdims=True)
        gain = ogain_ref[:, pl.ds(pl.multiple_of(source * local, local), local)]
        scaled = (part * gain).astype(jnp.bfloat16)
        product = jnp.dot(
            scaled, proj[pl.ds(pl.multiple_of(source * local, local), local), :], preferred_element_type=jnp.float32
        )
        if j == 0:
            stream[...] = product
        else:
            stream[...] += product
    inv_rms = lax.rsqrt(squares / (NX * local) + eps_norm)

    step_rows = 16
    for n in range(tokens // step_rows):
        part = slice(n * step_rows, (n + 1) * step_rows)
        value = alpha_mix * res_ref[part, :].astype(jnp.float32) + stream[part, :] * inv_rms[part, :]
        value = norm_rows(value, mgain_ref[...], mbias_ref[...]).astype(jnp.bfloat16)
        for c in range(chunks):
            mid[c * tokens + n * step_rows : c * tokens + (n + 1) * step_rows, :] = value[:, c * WIDE : (c + 1) * WIDE]

    def exchange(g, source, target, sends, receives, sign):
        for n in range(g * PER_GROUP, (g + 1) * PER_GROUP):
            dz, dy, dc, dx = ORDER[n]
            if not any(ORDER[n]):
                continue
            at = pl.ds(n * block, block)
            pltpu.make_async_remote_copy(
                src_ref=source.at[at, :],
                dst_ref=target.at[at, :],
                send_sem=sends.at[g],
                recv_sem=receives.at[g],
                device_id=(zs[sign * dz % NZ] + ys[sign * dy % NY] + cs[dc], xs_at[sign * dx % NX]),
                device_id_type=MESH,
            ).start()

    for g in range(GROUPS):
        sent[g * group_rows : (g + 1) * group_rows, :] = jnp.dot(
            choose[g * group_rows : (g + 1) * group_rows, :], mid[...], preferred_element_type=jnp.float32
        ).astype(jnp.bfloat16)
        exchange(g, sent, got, go_send, go_recv, 1)

    own_block = slice((DEVICES - 1) * block, DEVICES * block)
    got[own_block, :] = sent[own_block, :]
    for load in last_loads[1:]:
        load.wait()

    def whole(ref, g):
        return ref.at[pl.ds(g * group_rows, group_rows - (block if g == GROUPS - 1 else 0)), :]

    sub = 256
    ii = lax.broadcasted_iota(jnp.int32, (sub, sub), 0)
    jj = lax.broadcasted_iota(jnp.int32, (sub, sub), 1)
    per_chunk = sub // chunks

    def spot(i):
        return ((i % per_chunk) // CAP) * block + (i // per_chunk) * CAP + i % CAP

    collect = (jj == spot(ii)).astype(jnp.float32).astype(jnp.bfloat16)
    scatter = (ii == spot(jj)).astype(jnp.float32).astype(jnp.bfloat16)
    for g in range(GROUPS):
        pltpu.make_async_copy(whole(got, g), whole(got, g), go_recv.at[g]).wait()
        for s in range(group_rows // sub):
            ordered = jnp.dot(
                collect, got[g * group_rows + s * sub : g * group_rows + (s + 1) * sub, :], preferred_element_type=jnp.float32
            ).astype(jnp.bfloat16)
            for c in range(chunks):
                xs[s * per_chunk : (s + 1) * per_chunk, c * WIDE : (c + 1) * WIDE] = ordered[
                    c * per_chunk : (c + 1) * per_chunk, :
                ]
        x = xs[0 : PER_GROUP * CAP, :]
        gate_part = jnp.dot(x, gate[...], preferred_element_type=jnp.float32)
        up_part = jnp.dot(x, up[...], preferred_element_type=jnp.float32)
        hidden = (gate_part / (1.0 + jnp.exp(-gate_part)) * up_part).astype(jnp.bfloat16)
        result = jnp.dot(hidden, down[...], preferred_element_type=jnp.float32).astype(jnp.bfloat16)
        for s in range(group_rows // sub):
            stacked = jnp.concatenate(
                [result[s * per_chunk : (s + 1) * per_chunk, c * WIDE : (c + 1) * WIDE] for c in range(chunks)], axis=0
            )
            served[g * group_rows + s * sub : g * group_rows + (s + 1) * sub, :] = jnp.dot(
                scatter, stacked, preferred_element_type=jnp.float32
            ).astype(jnp.bfloat16)

        exchange(g, served, back, ret_send, ret_recv, -1)

    back[own_block, :] = served[own_block, :]

    for g in range(GROUPS):
        pltpu.make_async_copy(whole(back, g), whole(back, g), ret_recv.at[g]).wait()
        lanes = lax.broadcasted_iota(jnp.int32, (tokens, group_rows), 1) + g * group_rows
        arrived = back[g * group_rows : (g + 1) * group_rows, :]
        for c in range(chunks):
            total = jnp.zeros((tokens, WIDE), jnp.float32)
            for k in (0, 1):
                mine = (lanes == slot_columns[k, :, 0:1] + CAP * c).astype(jnp.float32).astype(jnp.bfloat16)
                total = total + weight_columns[k, :, 0:1] * jnp.dot(mine, arrived, preferred_element_type=jnp.float32)
            if g == 0:
                picked[:, c * WIDE : (c + 1) * WIDE] = total
            else:
                picked[:, c * WIDE : (c + 1) * WIDE] += total

    for n in range(tokens // step_rows):
        part = slice(n * step_rows, (n + 1) * step_rows)
        value = jnp.concatenate(
            [mid[c * tokens + n * step_rows : c * tokens + (n + 1) * step_rows, :] for c in range(chunks)], axis=1
        )
        value = alpha_mix * value.astype(jnp.float32) + picked[part, :]
        out_ref[part, :] = norm_rows(value, fgain_ref[...], fbias_ref[...]).astype(jnp.bfloat16)

    for copy in copies:
        copy.wait_send()
    for g in range(GROUPS):
        pltpu.make_async_copy(whole(sent, g), whole(sent, g), go_send.at[g]).wait()
        pltpu.make_async_copy(whole(served, g), whole(served, g), ret_send.at[g]).wait()
    for number in range(len(SENDS)):
        sent_copy(number).wait_send()
    for number, event in enumerate(list(OWN) + EVENTS):
        pair_copy(event, number).wait_send()


def per_device(
    queries, key_heads, value_heads, documents, query_gain, key_gain, out_gain, out_proj, residual, mid_gain, mid_bias,
    routes, route_weights, expert_gate, expert_up, expert_down, final_gain, final_bias,
):
    rows = queries.shape[0]
    heads = queries.shape[1] // HEAD
    tokens, width = residual.shape
    chunks = width // WIDE
    slots = DEVICES * CAP * chunks
    vec = lambda v: v.reshape(1, -1)
    tables = [jnp.asarray(t) for t in table_constants()]
    inputs = (
        queries, key_heads, value_heads, vec(documents), vec(query_gain), vec(key_gain), *tables,
        residual, routes.T, route_weights.T, jnp.asarray(order_table()), vec(out_gain), vec(mid_gain), vec(mid_bias),
        vec(final_gain), vec(final_bias), out_proj, expert_gate, expert_up, expert_down,
    )
    held = [v for n, v in enumerate(inputs) if n != 2]
    f32, bf16, i32 = jnp.float32, jnp.bfloat16, jnp.int32
    dma = pltpu.SemaphoreType.DMA
    return pl.pallas_call(
        layer_kernel,
        out_shape=jax.ShapeDtypeStruct((tokens, width), bf16),
        in_specs=[ANY] * len(inputs),
        out_specs=VMEM,
        scratch_shapes=[pltpu.VMEM(v.shape[-2:], v.dtype) for v in held]
        + [
            pltpu.VMEM((len(UNITS), NC, HALF_ROWS, 2 * HEAD), bf16),
            pltpu.VMEM((heads, rows, HEAD + DOC_ROWS), bf16),
            pltpu.VMEM((heads, rows, HEAD), f32),
            pltpu.VMEM((heads, rows, HEAD), f32),
            pltpu.VMEM((heads, rows, HEAD), f32),
            pltpu.VMEM((2, tokens, DEVICES), i32),
            pltpu.VMEM((2, tokens, DEVICES), f32),
            pltpu.VMEM((2, 8, tokens), i32),
            pltpu.VMEM((slots, chunks * tokens), bf16),
            pltpu.VMEM((rows, heads * HEAD), bf16),
            pltpu.VMEM((NX, tokens, heads * HEAD), bf16),
            pltpu.VMEM((tokens, width), f32),
            pltpu.VMEM((chunks * tokens, WIDE), bf16),
            pltpu.VMEM((slots, WIDE), bf16),
            pltpu.VMEM((slots, WIDE), bf16),
            pltpu.VMEM((slots, WIDE), bf16),
            pltpu.VMEM((slots, WIDE), bf16),
            pltpu.VMEM((tokens, width), f32),
            pltpu.VMEM((tokens, width), bf16),
            dma((len(inputs) + 3,)),
            dma((len(SENDS),)),
            dma((len(EVENTS),)),
            dma((len(EVENTS) + 2,)),
            dma((len(UNITS),)),
            dma((NX,)),
            dma((NX,)),
            dma((GROUPS,)),
            dma((GROUPS,)),
            dma((GROUPS,)),
            dma((GROUPS,)),
        ],
        compiler_params=pltpu.CompilerParams(
            collective_id=0, has_side_effects=True, vmem_limit_bytes=60 * 1024 * 1024
        ),
        name="layer",
    )(*inputs)


def solution(mesh):
    both = ("sp", "tp")
    return jax.shard_map(
        per_device,
        mesh=mesh,
        in_specs=(
            P("sp", "tp"),
            P("sp", "tp"),
            P("sp", "tp"),
            P("sp"),
            P(),
            P(),
            P(),
            P(),
            P(both, None),
            P(),
            P(),
            P(both, None),
            P(both, None),
            P(both, None, None),
            P(both, None, None),
            P(both, None, None),
            P(),
            P(),
        ),
        out_specs=P(both, None),
        check_vma=False,
    )
```
